32 devices in a mesh: sp: 8 (over z, y), tp: 4 (over x, core).
Axes of the slice: x: 2, y: 2, z: 4, core: 2. Of those that a mesh axis runs over, the one named last changes fastest.
Arguments:
- queries: bfloat16 [2304, 2048], P('sp', 'tp'), as said below
- key_vectors: bfloat16 [2304, 2048], P('sp', 'tp'), as said below
- latents: bfloat16 [2304, 2048], P('sp'), as said below
- value_weight: bfloat16 [2048, 2048], P(None, 'tp'), as said below
- log_sums: float32 [2304, 32], P('sp', 'tp'), as said below
- out_first: bfloat16 [2304, 2048], P('sp', 'tp'), as said below
- out_second: bfloat16 [2304, 2048], P('sp', 'tp'), as said below
- cotangent: bfloat16 [2304, 2048], P('sp', 'tp'), may hold values from -6 to 6
- head_lambda: float32 [16], P('tp'), may hold values from 0.3 to 0.8
Outputs:
- grad_queries: float32 [2304, 2048], P('sp', 'tp')
- grad_keys: float32 [2304, 2048], P('sp', 'tp')
- grad_latents: bfloat16 [2304, 2048], P('sp', 'tp')
- grad_weight: float32 [2048, 2048], P('sp', 'tp')
The draws below stay inside these ranges and needn't reach their ends.
Inputs may be any that keep to these rules, and one draw needn't show every extreme that they name: queries with entries of standard deviation 1.75. `key_vectors`: keys with entries of standard deviation 1. `latents`: inputs of standard deviation 1. `value_weight`: weights scaled by the inverse square root of 2048. `log_sums`: each row's log-sum of exponentials of its causal scores, for the given queries and keys. `out_first`: the first map's attention output for the given queries, keys, values and log-sums. `out_second`: the second map's attention output, likewise.
All inputs are finite; a program needn't handle non-finite values.
Results may differ from the reference program's by a relative error of at most 0.022.
Values may be sent and summed in bfloat16 or wider, within the bound.
A program may use at most 192 MiB of HBM per device.

```python
import jax
import jax.numpy as jnp
from jax import lax

D = 2048
HEADS = 16
DH = 64
DV = 128
TOK_DEV = 288
TOKENS = 2304
N_SP = 8
N_TP = 4


def build_inputs(key):
    queries = (1.75 * jax.random.normal(jax.random.fold_in(key, 101), (TOKENS, HEADS * 2 * DH), jnp.float32)).astype(jnp.bfloat16)
    key_vectors = jax.random.normal(jax.random.fold_in(key, 102), (TOKENS, HEADS * 2 * DH), jnp.float32).astype(jnp.bfloat16)
    latents = jax.random.normal(jax.random.fold_in(key, 103), (TOKENS, D), jnp.float32).astype(jnp.bfloat16)
    value_weight = (jax.random.normal(jax.random.fold_in(key, 104), (D, HEADS * DV), jnp.float32) * D ** (-0.5)).astype(jnp.bfloat16)
    values = jnp.dot(latents, value_weight, preferred_element_type=jnp.float32).astype(jnp.bfloat16)
    blocks = TOKENS // TOK_DEV
    query_heads = queries.astype(jnp.float32).reshape(blocks, TOK_DEV, HEADS, 2, DH)
    key_heads = key_vectors.astype(jnp.float32).reshape(TOKENS, HEADS, 2, DH)
    value_heads = values.astype(jnp.float32).reshape(TOKENS, HEADS, DV)
    positions = jnp.arange(TOKENS, dtype=jnp.int32)

    def one_block(pair):
        block_rows, block_index = pair
        query_pos = block_index * TOK_DEV + jnp.arange(TOK_DEV, dtype=jnp.int32)
        scores = jnp.einsum('nhad,mhad->hanm', block_rows, key_heads) * DH ** (-0.5)
        causal = query_pos[:, None] >= positions[None, :]
        scores = jnp.where(causal, scores, -1e+30)
        highest = jnp.max(scores, axis=-1, keepdims=True)
        expo = jnp.exp(scores - highest)
        total = jnp.sum(expo, axis=-1, keepdims=True)
        outputs = jnp.einsum('hanm,mhe->nhae', expo / total, value_heads)
        sums = (highest + jnp.log(total))[..., 0].transpose(2, 0, 1)
        return (sums, outputs)
    sums, outputs = lax.map(one_block, (query_heads, jnp.arange(blocks, dtype=jnp.int32)))
    log_sums = sums.reshape(TOKENS, HEADS * 2)
    out_first = outputs[:, :, :, 0, :].reshape(TOKENS, HEADS * DV).astype(jnp.bfloat16)
    out_second = outputs[:, :, :, 1, :].reshape(TOKENS, HEADS * DV).astype(jnp.bfloat16)
    return (queries, key_vectors, latents, value_weight, log_sums, out_first, out_second)


def draw_queries(key, part):
    return build_inputs(key)[0]


def draw_key_vectors(key, part):
    return build_inputs(key)[1]


def draw_latents(key, part):
    return build_inputs(key)[2]


def draw_value_weight(key, part):
    return build_inputs(key)[3]


def draw_log_sums(key, part):
    return build_inputs(key)[4]


def draw_out_first(key, part):
    return build_inputs(key)[5]


def draw_out_second(key, part):
    return build_inputs(key)[6]


def strengthened(entries, key, source, target, shards_of, factor):
    def block_of(dim):
        return (jnp.arange(entries.shape[dim]) // (entries.shape[dim] // shards_of)).reshape((-1,) + (1,) * (entries.ndim - 1 - dim))

    one_side = jax.random.permutation(key, shards_of)[block_of(target)]
    far = (block_of(target) + shards_of // 2) % shards_of
    return jnp.where((block_of(source) == one_side) | (block_of(source) == far), factor * entries, entries)


def block_scale(key, extent, shards, least, largest):
    factor_of = 1.0
    for dim, blocks in shards:
        steps = jax.random.uniform(jax.random.fold_in(jax.random.fold_in(key, 6), dim), (blocks,), jnp.float32, least / len(shards), largest / len(shards))
        factor_of = factor_of * jnp.repeat(jnp.exp(steps), extent[dim] // blocks).reshape((-1,) + (1,) * (len(extent) - 1 - dim))
    return factor_of


def noise_with(own_key, extent, spread, limit, cuts, heavy, kind=jnp.bfloat16):
    result = spread * jax.random.normal(own_key, extent, jnp.float32)
    if cuts:
        result = result * block_scale(own_key, extent, cuts, -0.22, 0.18)
    return jnp.clip(strengthened(result, jax.random.fold_in(own_key, 3), *heavy), -limit, limit).astype(kind)


def setup_inputs(seed: int = 0) -> dict:
    arg_keys = jax.random.split(jax.random.key(seed), 10)
    return {
        "queries": draw_queries(jax.random.fold_in(arg_keys[9], 71), 0),
        "key_vectors": draw_key_vectors(jax.random.fold_in(arg_keys[9], 71), 0),
        "latents": draw_latents(jax.random.fold_in(arg_keys[9], 71), 0),
        "value_weight": draw_value_weight(jax.random.fold_in(arg_keys[9], 71), 0),
        "log_sums": draw_log_sums(jax.random.fold_in(arg_keys[9], 71), 0),
        "out_first": draw_out_first(jax.random.fold_in(arg_keys[9], 71), 0),
        "out_second": draw_out_second(jax.random.fold_in(arg_keys[9], 71), 0),
        "cotangent": noise_with(arg_keys[7], (TOKENS, HEADS * DV), 1.0, 6.0, ((0, 8), (1, 4)), (0, 1, 8, 2.0)),
        "head_lambda": jnp.clip(0.3 + 0.5 * jax.random.uniform(arg_keys[8], (HEADS,), jnp.float32) ** block_scale(arg_keys[8], (HEADS,), ((0, 4),), -0.2, 0.2), 0.3, 0.8),
    }


def row_terms(out_first, out_second, cotangent, head_lambda):
    count = out_first.shape[0]
    head_count = head_lambda.shape[0]
    first = out_first.astype(jnp.float32).reshape(count, head_count, DV)
    second = out_second.astype(jnp.float32).reshape(count, head_count, DV)
    mixed = first - head_lambda[None, :, None] * second
    inverse = lax.rsqrt(lax.optimization_barrier(jnp.mean(mixed * mixed, axis=-1, keepdims=True)) + 1e-06)
    normed = mixed * inverse
    grad_out = cotangent.astype(jnp.float32).reshape(count, head_count, DV)
    grad_mixed = inverse * (grad_out - normed * lax.optimization_barrier(jnp.mean(grad_out * normed, axis=-1, keepdims=True)))
    grad_rows = grad_mixed.astype(jnp.bfloat16)
    widened = lax.optimization_barrier(grad_rows).astype(jnp.float32)
    row_dots = jnp.stack([lax.optimization_barrier(jnp.sum(widened * first, axis=-1)), lax.optimization_barrier(jnp.sum(widened * second, axis=-1))], axis=-1)
    return (grad_rows.reshape(count, head_count * DV), row_dots.reshape(count, head_count * 2))

def block_grads(query_rows, grad_rows, lse_rows, dot_rows, query_pos, key_rows, value_rows, key_pos, head_lambda):
    count = query_rows.shape[0]
    width = key_rows.shape[0]
    head_count = head_lambda.shape[0]
    score_scale = DH ** (-0.5)
    query_heads = query_rows.astype(jnp.float32).reshape(count, head_count, 2, DH)
    key_heads = key_rows.astype(jnp.float32).reshape(width, head_count, 2, DH)
    grad_heads = grad_rows.astype(jnp.float32).reshape(count, head_count, DV)
    value_heads = value_rows.astype(jnp.float32).reshape(width, head_count, DV)
    scores = jnp.einsum('nhad,mhad->hanm', query_heads, key_heads) * score_scale
    causal = query_pos[:, None] >= key_pos[None, :]
    shifts = lse_rows.reshape(count, head_count, 2).transpose(1, 2, 0)[..., None]
    probs = jnp.exp(jnp.where(causal, scores - shifts, -1e+30))
    d_attn = jnp.einsum('nhe,mhe->hnm', grad_heads, value_heads)
    dots = dot_rows.reshape(count, head_count, 2).transpose(1, 2, 0)[..., None]
    map_weight = jnp.stack([jnp.ones_like(head_lambda), -head_lambda], axis=1)[:, :, None, None]
    d_scores = (map_weight * probs * (d_attn[:, None] - dots)).astype(jnp.bfloat16)
    d_scores = lax.optimization_barrier(d_scores).astype(jnp.float32)
    weights = (probs[:, 0] - head_lambda[:, None, None] * probs[:, 1]).astype(jnp.bfloat16)
    weights = lax.optimization_barrier(weights).astype(jnp.float32)
    grad_q = jnp.einsum('hanm,mhad->nhad', d_scores, key_heads) * score_scale
    grad_k = jnp.einsum('hanm,nhad->mhad', d_scores, query_heads) * score_scale
    grad_v = jnp.einsum('hnm,nhe->mhe', weights, grad_heads)
    return (grad_q.reshape(count, -1), grad_k.reshape(width, -1), grad_v.reshape(width, -1))

def reference(queries, key_vectors, latents, value_weight, log_sums, out_first, out_second, cotangent, head_lambda):
    values = jnp.dot(latents, value_weight, preferred_element_type=jnp.float32).astype(jnp.bfloat16)
    grad_rows, row_dots = row_terms(out_first, out_second, cotangent, head_lambda)
    positions = jnp.arange(TOKENS, dtype=jnp.int32)

    def per_head(index):
        query_head = lax.dynamic_slice_in_dim(queries, index * 2 * DH, 2 * DH, 1)
        key_head = lax.dynamic_slice_in_dim(key_vectors, index * 2 * DH, 2 * DH, 1)
        value_head = lax.dynamic_slice_in_dim(values, index * DV, DV, 1)
        grad_head = lax.dynamic_slice_in_dim(grad_rows, index * DV, DV, 1)
        lse_head = lax.dynamic_slice_in_dim(log_sums, index * 2, 2, 1)
        dot_head = lax.dynamic_slice_in_dim(row_dots, index * 2, 2, 1)
        lambda_one = lax.dynamic_slice_in_dim(head_lambda, index, 1, 0)

        def block_step(totals, block_index):
            first_row = (block_index * TOK_DEV).astype(jnp.int32)
            query_pos = first_row + jnp.arange(TOK_DEV, dtype=jnp.int32)
            grad_q, grad_k, grad_v = block_grads(lax.dynamic_slice_in_dim(query_head, first_row, TOK_DEV, 0), lax.dynamic_slice_in_dim(grad_head, first_row, TOK_DEV, 0), lax.dynamic_slice_in_dim(lse_head, first_row, TOK_DEV, 0), lax.dynamic_slice_in_dim(dot_head, first_row, TOK_DEV, 0), query_pos, key_head, value_head, positions, lambda_one)
            return ((totals[0] + grad_k, totals[1] + grad_v), grad_q)
        initial = (jnp.zeros((TOKENS, 2 * DH), jnp.float32), jnp.zeros((TOKENS, DV), jnp.float32))
        totals, grad_blocks = lax.scan(block_step, initial, jnp.arange(N_SP, dtype=jnp.int32))
        return (grad_blocks.reshape(TOKENS, 2 * DH), totals[0], totals[1])
    grad_q, grad_k, grad_v = lax.map(per_head, jnp.arange(HEADS, dtype=jnp.int32))
    grad_queries = grad_q.transpose(1, 0, 2).reshape(TOKENS, HEADS * 2 * DH)
    grad_keys = grad_k.transpose(1, 0, 2).reshape(TOKENS, HEADS * 2 * DH)
    grad_values = grad_v.transpose(1, 0, 2).reshape(TOKENS, HEADS * DV).astype(jnp.bfloat16)
    grad_weight = lax.dot_general(latents, grad_values, (((0,), (0,)), ((), ())), preferred_element_type=jnp.float32)
    value_groups = grad_values.reshape(TOKENS, N_TP, -1).transpose(1, 0, 2)
    weight_groups = value_weight.reshape(D, N_TP, -1).transpose(1, 0, 2)

    def add_group(total, pair):
        partial_sum = lax.dot_general(pair[0], pair[1], (((1,), (1,)), ((), ())), preferred_element_type=jnp.float32)
        rounded = lax.optimization_barrier(partial_sum.astype(jnp.bfloat16))
        return (total + rounded.astype(jnp.float32), None)
    latent_total, unused = lax.scan(add_group, jnp.zeros((TOKENS, D), jnp.float32), (value_groups, weight_groups))
    return (grad_queries, grad_keys, latent_total.astype(jnp.bfloat16), grad_weight)
```

```python
import functools

import jax
import jax.numpy as jnp
from jax import lax
from jax.experimental import pallas as pl
from jax.experimental.pallas import tpu as pltpu
from jax.sharding import PartitionSpec as P

DH = 64
DV = 128
BLOCK = 256


def row_terms(out_first, out_second, cotangent, head_lambda):
    count = out_first.shape[0]
    head_count = head_lambda.shape[0]
    first = out_first.astype(jnp.float32).reshape(count, head_count, DV)
    second = out_second.astype(jnp.float32).reshape(count, head_count, DV)
    mixed = first - head_lambda[None, :, None] * second
    inverse = lax.rsqrt(jnp.mean(mixed * mixed, axis=-1, keepdims=True) + 1e-06)
    normed = mixed * inverse
    grad_out = cotangent.astype(jnp.float32).reshape(count, head_count, DV)
    grad_mixed = inverse * (grad_out - normed * jnp.mean(grad_out * normed, axis=-1, keepdims=True))
    grad_rows = grad_mixed.astype(jnp.bfloat16)
    widened = lax.optimization_barrier(grad_rows).astype(jnp.float32)
    row_dots = jnp.stack(
        [jnp.sum(widened * first, axis=-1), jnp.sum(widened * second, axis=-1)], axis=-1
    )
    return (grad_rows.reshape(count, head_count * DV), row_dots.reshape(count, head_count * 2))


def block_grads(
    query_rows, grad_rows, lse_rows, dot_rows, query_pos, key_rows, value_rows, key_pos, head_lambda
):
    count = query_rows.shape[0]
    width = key_rows.shape[0]
    head_count = head_lambda.shape[0]
    score_scale = DH ** (-0.5)
    query_heads = query_rows.reshape(count, head_count, 2, DH)
    key_heads = key_rows.reshape(width, head_count, 2, DH)
    grad_heads = grad_rows.reshape(count, head_count, DV)
    value_heads = value_rows.reshape(width, head_count, DV)
    scores = (
        jnp.einsum("nhad,mhad->hanm", query_heads, key_heads, preferred_element_type=jnp.float32)
        * score_scale
    )
    causal = query_pos[:, None] >= key_pos[None, :]
    shifts = lse_rows.reshape(count, head_count, 2).transpose(1, 2, 0)[..., None]
    probs = jnp.exp(jnp.where(causal, scores - shifts, -1e30))
    d_attn = jnp.einsum("nhe,mhe->hnm", grad_heads, value_heads, preferred_element_type=jnp.float32)
    dots = dot_rows.reshape(count, head_count, 2).transpose(1, 2, 0)[..., None]
    map_weight = jnp.stack([jnp.ones_like(head_lambda), -head_lambda], axis=1)[:, :, None, None]
    d_scores = (map_weight * probs * (d_attn[:, None] - dots)).astype(jnp.bfloat16)
    weights = (probs[:, 0] - head_lambda[:, None, None] * probs[:, 1]).astype(jnp.bfloat16)
    grad_q = (
        jnp.einsum("hanm,mhad->nhad", d_scores, key_heads, preferred_element_type=jnp.float32)
        * score_scale
    )
    grad_k = (
        jnp.einsum("hanm,nhad->mhad", d_scores, query_heads, preferred_element_type=jnp.float32)
        * score_scale
    )
    grad_v = jnp.einsum("hnm,nhe->mhe", weights, grad_heads, preferred_element_type=jnp.float32)
    return (grad_q.reshape(count, -1), grad_k.reshape(width, -1), grad_v.reshape(width, -1))


def per_device(
    queries,
    key_vectors,
    latents,
    value_weight,
    log_sums,
    out_first,
    out_second,
    cotangent,
    head_lambda,
):
    local_rows = queries.shape[0]
    offset = lax.axis_index("sp") * local_rows
    positions = offset + jnp.arange(local_rows, dtype=jnp.int32)
    last_row = offset + local_rows - 1
    values = jnp.dot(latents, value_weight, preferred_element_type=jnp.float32).astype(jnp.bfloat16)
    grad_rows, row_dots = row_terms(out_first, out_second, cotangent, head_lambda)
    gathered_stats = (
        lax.all_gather(log_sums, "sp", axis=0, tiled=True),
        lax.all_gather(row_dots, "sp", axis=0, tiled=True),
    )
    key_rows = lax.all_gather(key_vectors, "sp", axis=0, tiled=True)
    value_rows = lax.all_gather(values, "sp", axis=0, tiled=True)
    count = key_rows.shape[0]

    def compute(current):
        key_pos = jnp.arange(count, dtype=jnp.int32)
        grad_q, unused_k, unused_v = block_grads(
            queries,
            grad_rows,
            log_sums,
            row_dots,
            positions,
            key_rows,
            value_rows,
            key_pos,
            head_lambda,
        )
        return grad_q

    grad_queries = lax.cond(
        jnp.int32(0) <= last_row,
        compute,
        lambda current: current,
        jnp.zeros((local_rows, queries.shape[1]), jnp.float32),
    )
    start_totals = (
        jnp.zeros((local_rows, key_vectors.shape[1]), jnp.float32),
        jnp.zeros((local_rows, values.shape[1]), jnp.float32),
    )
    query_rows = lax.all_gather(queries, "sp", axis=0, tiled=True)
    grad_piece = lax.all_gather(grad_rows, "sp", axis=0, tiled=True)
    add_count = query_rows.shape[0]

    def compute(current):
        query_pos = jnp.arange(add_count, dtype=jnp.int32)
        lse_rows = gathered_stats[0]
        dot_rows = gathered_stats[1]
        unused_q, grad_k, grad_v = block_grads(
            query_rows,
            grad_piece,
            lse_rows,
            dot_rows,
            query_pos,
            key_vectors,
            values,
            positions,
            head_lambda,
        )
        return (grad_k, grad_v)

    grad_keys, grad_values = lax.cond(
        jnp.int32(0) + add_count - 1 >= offset, compute, lambda current: current, start_totals
    )
    values_grad = grad_values.astype(jnp.bfloat16)
    grad_weight = lax.psum_scatter(
        lax.dot_general(
            latents, values_grad, (((0,), (0,)), ((), ())), preferred_element_type=jnp.float32
        ).astype(jnp.bfloat16),
        "sp",
        scatter_dimension=0,
        tiled=True,
    ).astype(jnp.float32)
    latent_partial = lax.dot_general(
        values_grad, value_weight, (((1,), (1,)), ((), ())), preferred_element_type=jnp.float32
    )
    grad_latents = lax.psum_scatter(
        latent_partial.astype(jnp.bfloat16), "tp", scatter_dimension=1, tiled=True
    )
    return (grad_queries, grad_keys, grad_latents, grad_weight)


def level(z, k, nz):
    bit, out = 1, z
    while bit < nz:
        out = out + ((k // bit) % 2) * bit * (1 - 2 * ((z // bit) % 2))
        bit *= 2
    return out


def lanes(index, width=DV):
    return pl.ds(pl.multiple_of(index * width, width), width)


def chunk(index, rows):
    return pl.ds(pl.multiple_of(index * rows, rows), rows)


def pad_tiles(rows, block=BLOCK):
    return -(-rows // block)


def remote(src, dst, send_sem, recv_sem, where):
    return pltpu.make_async_remote_copy(
        src_ref=src,
        dst_ref=dst,
        send_sem=send_sem,
        recv_sem=recv_sem,
        device_id=where,
        device_id_type=pl.DeviceIdType.MESH,
    )


def greet(devices):
    barrier = pltpu.get_barrier_semaphore()
    for device in devices:
        pl.semaphore_signal(
            barrier, inc=1, device_id=device, device_id_type=pl.DeviceIdType.MESH
        )
    return lambda: pl.semaphore_wait(barrier, len(devices))


NT = (((1,), (1,)), ((), ()))
TN = (((0,), (0,)), ((), ()))


def forward_kernel(
    nz, q_ref, k_ref, lat_ref, w_ref, first_ref, second_ref, cot_ref, lse_ref, lambda_ref,
    dq_ref, dkm_ref, dvm_ref, dko_ref, dvo_ref, latp_ref,
    first_s, second_s, cot_s, lat_s, w_s, grad_s, stat_s, v_s,
    q_all, do_all, k_all, v_all, stat_r, q0_s, q1_s, stat_t, dqt_s, dk_s, dv_s,
    load_sem, own_sem, send_sem, recv_sem, pass_send, pass_recv, lat_send, lat_recv
):
    sp = lax.axis_index("sp")
    z, y = sp // 2, lax.rem(sp, 2)
    rows = q_ref.shape[0]
    width = latp_ref.shape[2]
    tiles = stat_t.shape[0]
    partner = {"sp": 2 * z + 1 - y}
    peers = [{"sp": 2 * level(z, k, nz) + y} for k in range(1, nz)]
    loads = [
        pltpu.make_async_copy(src, dst, load_sem.at[i])
        for i, (src, dst) in enumerate(
            [(first_ref, first_s), (second_ref, second_s), (cot_ref, cot_s),
             (lat_ref, lat_s), (w_ref, w_s)]
        )
    ]
    for load in loads:
        load.start()
    arrived = greet(peers + [partner])
    own_q = pltpu.make_async_copy(q_ref.at[:, lanes(z)], q_all.at[chunk(z, rows)], own_sem.at[0])
    own_k = pltpu.make_async_copy(k_ref.at[:, lanes(z)], k_all.at[chunk(sp, rows)], own_sem.at[1])
    own_q.start()
    own_k.start()
    tail = q_all.shape[0] - nz * rows
    q_all[nz * rows :, :] = jnp.zeros((tail, DV), jnp.bfloat16)
    do_all[nz * rows :, :] = jnp.zeros((tail, DV), jnp.bfloat16)
    dqt_s[...] = jnp.zeros_like(dqt_s)
    arrived()

    def send(part, k):
        where = peers[k - 1]
        to = level(z, k, nz)
        src, dst = {
            0: (q_ref.at[:, lanes(to)], q_all.at[chunk(z, rows)]),
            1: (grad_s.at[:, lanes(to)], do_all.at[chunk(z, rows)]),
            2: (stat_s.at[to], stat_r.at[z]),
            3: (k_ref.at[:, lanes(to)], k_all.at[chunk(sp, rows)]),
            4: (v_s.at[:, lanes(to)], v_all.at[chunk(sp, rows)]),
        }[part]
        return remote(src, dst, send_sem.at[part, k], recv_sem.at[part, k], where)

    def passed(part, k, src, at):
        dst = (k_all, v_all)[part].at[chunk(at, rows)]
        return remote(src, dst, pass_send.at[part, k], pass_recv.at[part, k], partner)

    def lat_copy(t):
        return remote(
            lat_ref.at[:, lanes(2 * t + 1 - y, width)], latp_ref.at[t],
            lat_send.at[t], lat_recv.at[t], partner
        )

    for k in range(1, nz):
        send(0, k).start()
    passed(0, 0, k_ref.at[:, lanes(z)], sp).start()
    for t in range(nz):
        lat_copy(t).start()

    for load in loads[:3]:
        load.wait()
    columns = []
    for head in range(nz):
        at = slice(head * DV, (head + 1) * DV)
        first = first_s[:, at].astype(jnp.float32)
        second = second_s[:, at].astype(jnp.float32)
        mixed = first - lambda_ref[head] * second
        inverse = lax.rsqrt(jnp.mean(mixed * mixed, axis=-1, keepdims=True) + 1e-06)
        normed = mixed * inverse
        grad_out = cot_s[:, at].astype(jnp.float32)
        mean_dot = jnp.mean(grad_out * normed, axis=-1, keepdims=True)
        grad_rows = (inverse * (grad_out - normed * mean_dot)).astype(jnp.bfloat16)
        grad_s[:, at] = grad_rows
        widened = grad_rows.astype(jnp.float32)
        columns.append(jnp.sum(widened * first, axis=-1, keepdims=True))
        columns.append(jnp.sum(widened * second, axis=-1, keepdims=True))
    dots = jnp.concatenate(columns, axis=1).T
    for head in range(nz):
        pair = slice(2 * head, 2 * head + 2)
        stat_s[head] = jnp.concatenate(
            [lse_ref[pair, :], dots[pair, :], jnp.zeros((4, rows), jnp.float32)], axis=0
        )
    for k in range(1, nz):
        send(2, k).start()
        send(1, k).start()
    own_do = pltpu.make_async_copy(grad_s.at[:, lanes(z)], do_all.at[chunk(z, rows)], own_sem.at[2])
    own_do.start()
    stat_r[z] = stat_s[z]
    for k in range(1, nz):
        send(3, k).start()
    for load in loads[3:]:
        load.wait()
    v_s[...] = jnp.dot(lat_s[...], w_s[...], preferred_element_type=jnp.float32).astype(
        jnp.bfloat16
    )
    for k in range(1, nz):
        send(4, k).start()
    own_v = pltpu.make_async_copy(v_s.at[:, lanes(z)], v_all.at[chunk(sp, rows)], own_sem.at[3])
    own_v.start()
    passed(1, 0, v_s.at[:, lanes(z)], sp).start()

    for part in range(3):
        for k in range(1, nz):
            send(part, k).wait_recv()
    own_q.wait()
    own_k.wait()
    own_do.wait()
    own_v.wait()
    scale = jnp.bfloat16(DH**-0.5)
    queries = q_all[...] * scale
    half = lax.broadcasted_iota(jnp.int32, queries.shape, 1) < DH
    q0_s[...] = jnp.where(half, queries, jnp.zeros_like(queries))
    q1_s[...] = jnp.where(half, jnp.zeros_like(queries), queries)
    stats = jnp.concatenate(
        [stat_r[c] for c in range(nz)] + [jnp.full((8, tail), 1e30, jnp.float32)], axis=1
    )
    for t in range(tiles):
        stat_t[t] = stats[:, t * BLOCK : (t + 1) * BLOCK]
    weight = lambda_ref[z]

    def column(j):
        key_rows = chunk(j, rows)
        keys = k_all[key_rows, :]
        keys_t = keys.T
        dk_s[...] = jnp.zeros_like(dk_s)
        dv_s[...] = jnp.zeros_like(dv_s)
        lowest = (j + 1 - y) // 2
        begin = (lowest * rows) // BLOCK
        middle = jnp.minimum(((lowest + 1) * rows - 1) // BLOCK + 1, tiles)
        begin = jnp.where(lowest == nz, tiles, begin)

        def tile(t, masked):
            at = chunk(t, BLOCK)
            q0, q1, grads = q0_s[at, :], q1_s[at, :], do_all[at, :]
            keys = k_all[key_rows, :]
            stat = stat_t[t]
            s0 = lax.dot_general(keys, q0, NT, preferred_element_type=jnp.float32)
            s1 = lax.dot_general(keys, q1, NT, preferred_element_type=jnp.float32)
            d_attn = lax.dot_general(
                v_all[key_rows, :], grads, NT, preferred_element_type=jnp.float32
            )
            x0 = s0 - stat[0:1, :]
            x1 = s1 - stat[1:2, :]
            if masked:
                place = t * BLOCK + lax.broadcasted_iota(jnp.int32, (1, BLOCK), 1)
                shift = y * rows - j * rows + place
                for c in range(1, nz):
                    shift = shift + jnp.where(place >= c * rows, rows, 0)
                seen = lax.broadcasted_iota(jnp.int32, (rows, BLOCK), 0) <= shift
                x0 = jnp.where(seen, x0, -1e30)
                x1 = jnp.where(seen, x1, -1e30)
            p0 = jnp.exp(x0)
            p1 = weight * jnp.exp(x1)
            ds0 = (p0 * (d_attn - stat[2:3, :])).astype(jnp.bfloat16)
            ds1 = (p1 * (stat[3:4, :] - d_attn)).astype(jnp.bfloat16)
            w = (p0 - p1).astype(jnp.bfloat16)
            dk_s[...] += jnp.dot(ds0, q0, preferred_element_type=jnp.float32) + jnp.dot(
                ds1, q1, preferred_element_type=jnp.float32
            )
            dv_s[...] += jnp.dot(w, grads, preferred_element_type=jnp.float32)
            dqt_s[t, :DH, :] += jnp.dot(keys_t[:DH], ds0, preferred_element_type=jnp.float32)
            dqt_s[t, DH:, :] += jnp.dot(keys_t[DH:], ds1, preferred_element_type=jnp.float32)

        def first_tiles(t, carry):
            tile(t, True)
            return carry

        def other_tiles(t, carry):
            tile(t, False)
            return carry

        lax.fori_loop(begin, middle, first_tiles, 0)
        lax.fori_loop(jnp.maximum(begin, middle), tiles, other_tiles, 0)

    def step(i, carry):
        k, side = i // 2, i % 2
        at = level(z, k, nz)
        mine = 2 * at + y

        @pl.when(side == 0)
        def _():
            @pl.when(k > 0)
            def _():
                for part, kept in ((3, k_all), (4, v_all)):
                    remote(
                        kept.at[chunk(mine, rows)], kept.at[chunk(mine, rows)],
                        send_sem.at[part, k], recv_sem.at[part, k], {"sp": mine}
                    ).wait_recv()
                    passed(part - 3, k, kept.at[chunk(mine, rows)], mine).start()

        @pl.when(side == 1)
        def _():
            for part, kept in ((0, k_all), (1, v_all)):
                other = 2 * at + 1 - y
                passed(part, k, kept.at[chunk(other, rows)], other).wait_recv()

        column(2 * at + (y + side) % 2)

        @pl.when(side == 0)
        def _():
            dkm_ref[at] = dk_s[...]
            dvm_ref[at] = dv_s[...]

        @pl.when(side == 1)
        def _():
            dko_ref[at] = dk_s[...].astype(jnp.bfloat16)
            dvo_ref[at] = dv_s[...].astype(jnp.bfloat16)

        return carry

    lax.fori_loop(0, 2 * nz, step, 0)
    for t in range(tiles):
        dq_ref[t * BLOCK : (t + 1) * BLOCK, :] = (dqt_s[t] * DH ** (-0.5)).T.astype(jnp.bfloat16)
    for t in range(nz):
        lat_copy(t).wait_recv()
        lat_copy(t).wait_send()
    for part in range(5):
        for k in range(1, nz):
            send(part, k).wait_send()
    for part in range(2):
        for k in range(nz):
            passed(part, k, (k_all, v_all)[part].at[chunk(sp, rows)], sp).wait_send()


def forward(queries, keys, latents, value_weight, first, second, cotangent, lse, head_lambda, n):
    rows = queries.shape[0]
    depth, wide = value_weight.shape
    nz = n // 2
    width = depth // n
    tiles = pad_tiles(nz * rows)
    dense = jnp.bfloat16
    vmem = pl.BlockSpec(memory_space=pltpu.VMEM)
    hbm = pl.BlockSpec(memory_space=pl.ANY)
    sem = pltpu.SemaphoreType.DMA
    piece = (nz, rows, DV)
    return pl.pallas_call(
        functools.partial(forward_kernel, nz),
        out_shape=[
            jax.ShapeDtypeStruct((tiles * BLOCK, DV), dense),
            jax.ShapeDtypeStruct(piece, jnp.float32),
            jax.ShapeDtypeStruct(piece, jnp.float32),
            jax.ShapeDtypeStruct(piece, dense),
            jax.ShapeDtypeStruct(piece, dense),
            jax.ShapeDtypeStruct((nz, rows, width), dense),
        ],
        in_specs=[hbm] * 7 + [vmem, pl.BlockSpec(memory_space=pltpu.SMEM)],
        out_specs=[vmem] * 6,
        scratch_shapes=[
            pltpu.VMEM((rows, wide), dense),
            pltpu.VMEM((rows, wide), dense),
            pltpu.VMEM((rows, wide), dense),
            pltpu.VMEM((rows, depth), dense),
            pltpu.VMEM((depth, wide), dense),
            pltpu.VMEM((rows, wide), dense),
            pltpu.VMEM((nz, 8, rows), jnp.float32),
            pltpu.VMEM((rows, wide), dense),
            pltpu.VMEM((tiles * BLOCK, DV), dense),
            pltpu.VMEM((tiles * BLOCK, DV), dense),
            pltpu.VMEM((n * rows, DV), dense),
            pltpu.VMEM((n * rows, DV), dense),
            pltpu.VMEM((nz, 8, rows), jnp.float32),
            pltpu.VMEM((tiles * BLOCK, DV), dense),
            pltpu.VMEM((tiles * BLOCK, DV), dense),
            pltpu.VMEM((tiles, 8, BLOCK), jnp.float32),
            pltpu.VMEM((tiles, 2 * DH, BLOCK), jnp.float32),
            pltpu.VMEM((rows, DV), jnp.float32),
            pltpu.VMEM((rows, DV), jnp.float32),
            sem((5,)),
            sem((4,)),
            sem((5, nz)),
            sem((5, nz)),
            sem((2, nz)),
            sem((2, nz)),
            sem((nz,)),
            sem((nz,)),
        ],
        compiler_params=pltpu.CompilerParams(collective_id=1, has_side_effects=True),
    )(queries, keys, latents, value_weight, first, second, cotangent, lse, head_lambda)


def back_kernel(
    nz, ntp, dq_ref, dkm_ref, dvm_ref, dko_ref, dvo_ref, latp_ref, lat_ref, w_ref,
    q_home, k_home, gl_ref, gw_ref,
    lat_s, w_s, dky_s, dvy_s, dks_s, dvs_s, v_pair, gl_send, gl_recv,
    up_send, up_recv, down_send, down_recv, sum_s,
    load_sem, own_sem, q_send, q_recv, y_send, y_recv, z_send, z_recv, h_send, h_recv,
    t_send, t_recv, u_send, u_recv, d_send, d_recv
):
    sp, tp = lax.axis_index("sp"), lax.axis_index("tp")
    z, y = sp // 2, lax.rem(sp, 2)
    rows = dkm_ref.shape[1]
    width = latp_ref.shape[2]
    parts = up_send.shape[1]
    piece = width // parts
    partner = {"sp": 2 * z + 1 - y}
    peers = [{"sp": 2 * level(z, k, nz) + y} for k in range(1, nz)]
    sides = [{"tp": lax.rem(tp + step, ntp)} for step in range(1, ntp)]
    lat_load = pltpu.make_async_copy(lat_ref, lat_s, load_sem.at[0])
    w_load = pltpu.make_async_copy(w_ref, w_s, load_sem.at[1])
    lat_load.start()
    w_load.start()
    arrived = greet(peers + [partner] + sides)
    own_q = pltpu.make_async_copy(
        dq_ref.at[chunk(z, rows)], q_home.at[:, lanes(z)], own_sem.at[0]
    )
    own_q.start()
    arrived()

    def q_copy(k):
        at = level(z, k, nz)
        return remote(
            dq_ref.at[chunk(at, rows)], q_home.at[:, lanes(z)],
            q_send.at[k], q_recv.at[k], peers[k - 1]
        )

    def y_copy(part, k):
        at = level(z, k, nz)
        src, dst = ((dvo_ref, dvy_s), (dko_ref, dky_s))[part]
        return remote(src.at[at], dst.at[at], y_send.at[part, k], y_recv.at[part, k], partner)

    def z_copy(part, k):
        at = level(z, k, nz)
        src = (dvs_s, dks_s)[part].at[at]
        dst = v_pair.at[0:rows, lanes(z)] if part == 0 else k_home.at[:, lanes(z)]
        return remote(src, dst, z_send.at[part, k], z_recv.at[part, k], peers[k - 1])

    def home_copy(k):
        head = level(z, k, nz)
        return remote(
            v_pair.at[0:rows, lanes(head)], v_pair.at[rows : 2 * rows, lanes(head)],
            h_send.at[k], h_recv.at[k], partner
        )

    order = list(range(1, nz)) + [0]
    for part in range(2):
        for k in order:
            y_copy(part, k).start()
    for k in range(1, nz):
        q_copy(k).start()
    for part, (mine, got, total) in enumerate(
        ((dvm_ref, dvy_s, dvs_s), (dkm_ref, dky_s, dks_s))
    ):
        for k in order:
            at = level(z, k, nz)
            y_copy(part, k).wait_recv()
            added = (mine[at] + got[at].astype(jnp.float32)).astype(jnp.bfloat16)
            if k == 0:
                if part == 0:
                    v_pair[0:rows, lanes(z)] = added
                else:
                    k_home[:, lanes(z)] = added
            else:
                total[at] = added
                z_copy(part, k).start()
    home_copy(0).start()
    for k in range(1, nz):
        z_copy(0, k).wait_recv()
        home_copy(k).start()

    w_load.wait()
    own_rows = v_pair[0:rows, :]
    wide = gl_ref.shape[1]

    def t_copy(step):
        return remote(
            gl_send.at[step], gl_recv.at[step], t_send.at[step], t_recv.at[step], sides[step - 1]
        )

    def latent_term(at):
        return lax.dot_general(
            own_rows, w_s[chunk(at, wide), :], NT, preferred_element_type=jnp.float32
        ).astype(jnp.bfloat16)

    for step in range(1, ntp):
        gl_send[step] = latent_term(lax.rem(tp + step, ntp))
        t_copy(step).start()
    gl_send[0] = latent_term(tp)
    lat_load.wait()
    for k in range(nz):
        home_copy(k).wait_recv()

    def term(t, s):
        at = pl.ds(pl.multiple_of((2 * t + y) * width + s * piece, piece), piece)
        own = lat_s[:, at]
        other = latp_ref[t, :, s * piece : (s + 1) * piece]
        return lax.dot_general(
            jnp.concatenate([own, other], axis=0), v_pair[...], TN,
            preferred_element_type=jnp.float32,
        )

    def line_copy(up, t, s):
        if up:
            return remote(
                up_send.at[t, s], up_recv.at[t, s], u_send.at[t, s], u_recv.at[t, s],
                {"sp": 2 * (z + 1) + y}
            )
        return remote(
            down_send.at[t, s], down_recv.at[t, s], d_send.at[t, s], d_recv.at[t, s],
            {"sp": 2 * (z - 1) + y}
        )

    hops = []
    for i in range(nz - 1):
        hops += [(True, nz - 1 - i), (False, i)]

    for up, t in hops:
        for s in range(parts):
            @pl.when((z < t) if up else (z > t))
            def _():
                sum_s[...] = term(t, s)

                @pl.when((z > 0) if up else (z < nz - 1))
                def _():
                    line_copy(up, t, s).wait_recv()
                    sum_s[...] += (up_recv if up else down_recv)[t, s].astype(jnp.float32)

                (up_send if up else down_send)[t, s] = sum_s[...].astype(jnp.bfloat16)
                line_copy(up, t, s).start()

    own_q.wait()
    total = gl_send[0].astype(jnp.float32)
    for step in range(1, ntp):
        t_copy(step).wait_recv()
        total = total + gl_recv[step].astype(jnp.float32)
    gl_ref[...] = total.astype(jnp.bfloat16)
    for s in range(parts):
        at = slice(s * piece, (s + 1) * piece)
        own = pl.ds(pl.multiple_of((2 * z + y) * width + s * piece, piece), piece)
        gw_ref[at, :] = lax.dot_general(
            jnp.concatenate([lat_s[:, own], latp_ref[z, :, at]], axis=0), v_pair[...], TN,
            preferred_element_type=jnp.float32,
        )
    for k in range(1, nz):
        q_copy(k).wait_recv()
        z_copy(1, k).wait_recv()
    for t in range(nz):
        for s in range(parts):
            at = slice(s * piece, (s + 1) * piece)
            if t > 0:
                @pl.when(z == t)
                def _():
                    line_copy(True, t, s).wait_recv()
                    gw_ref[at, :] += up_recv[t, s].astype(jnp.float32)
            if t < nz - 1:
                @pl.when(z == t)
                def _():
                    line_copy(False, t, s).wait_recv()
                    gw_ref[at, :] += down_recv[t, s].astype(jnp.float32)
    for up, t in hops:
        for s in range(parts):
            @pl.when((z < t) if up else (z > t))
            def _():
                line_copy(up, t, s).wait_send()
    for k in range(1, nz):
        q_copy(k).wait_send()
        for part in range(2):
            z_copy(part, k).wait_send()
    for k in range(nz):
        home_copy(k).wait_send()
        for part in range(2):
            y_copy(part, k).wait_send()
    for step in range(1, ntp):
        t_copy(step).wait_send()


def back(dq, dkm, dvm, dko, dvo, latp, latents, value_weight, ntp):
    nz, rows, _ = dkm.shape
    depth, wide = value_weight.shape
    width = latp.shape[2]
    parts = 2 if width % 256 == 0 else 1
    dense = jnp.bfloat16
    vmem = pl.BlockSpec(memory_space=pltpu.VMEM)
    hbm = pl.BlockSpec(memory_space=pl.ANY)
    sem = pltpu.SemaphoreType.DMA
    share = depth // ntp
    line = pltpu.VMEM((nz, parts, width // parts, wide), dense)
    return pl.pallas_call(
        functools.partial(back_kernel, nz, ntp),
        out_shape=[
            jax.ShapeDtypeStruct((rows, wide), dense),
            jax.ShapeDtypeStruct((rows, wide), dense),
            jax.ShapeDtypeStruct((rows, share), dense),
            jax.ShapeDtypeStruct((width, wide), jnp.float32),
        ],
        in_specs=[vmem] * 6 + [hbm] * 2,
        out_specs=[vmem] * 4,
        scratch_shapes=[
            pltpu.VMEM((rows, depth), dense),
            pltpu.VMEM((depth, wide), dense),
        ]
        + [pltpu.VMEM((nz, rows, DV), dense)] * 4
        + [
            pltpu.VMEM((2 * rows, wide), dense),
            pltpu.VMEM((ntp, rows, share), dense),
            pltpu.VMEM((ntp, rows, share), dense),
        ]
        + [line] * 4
        + [
            pltpu.VMEM((width // parts, wide), jnp.float32),
            sem((2,)),
            sem((1,)),
            sem((nz,)),
            sem((nz,)),
            sem((2, nz)),
            sem((2, nz)),
            sem((2, nz)),
            sem((2, nz)),
            sem((nz,)),
            sem((nz,)),
            sem((ntp,)),
            sem((ntp,)),
            sem((nz, parts)),
            sem((nz, parts)),
            sem((nz, parts)),
            sem((nz, parts)),
        ],
        compiler_params=pltpu.CompilerParams(collective_id=2, has_side_effects=True),
    )(dq, dkm, dvm, dko, dvo, latp, latents, value_weight)


def finish_kernel(q_ref, k_ref, gl_ref, gw_ref, q_out, k_out, gl_out, gw_out):
    q_out[...] = q_ref[...].astype(jnp.float32)
    k_out[...] = k_ref[...].astype(jnp.float32)
    gl_out[...] = gl_ref[...]
    gw_out[...] = gw_ref[...]


def finish(q_home, k_home, gl, gw):
    vmem = pl.BlockSpec(memory_space=pltpu.VMEM)
    kinds = ((q_home, jnp.float32), (k_home, jnp.float32), (gl, gl.dtype), (gw, gw.dtype))
    return pl.pallas_call(
        finish_kernel,
        out_shape=[jax.ShapeDtypeStruct(a.shape, kind) for a, kind in kinds],
        in_specs=[vmem] * 4,
        out_specs=[vmem] * 4,
    )(q_home, k_home, gl, gw)


def by_level(
    queries, key_vectors, latents, value_weight, log_sums, out_first, out_second, cotangent,
    head_lambda
):
    n, ntp = lax.axis_size("sp"), lax.axis_size("tp")
    *grads, latp = forward(
        queries, key_vectors, latents, value_weight, out_first, out_second, cotangent,
        log_sums.T, head_lambda, n
    )
    return tuple(finish(*back(*grads, latp, latents, value_weight, ntp)))


def dispatch(queries, key_vectors, latents, value_weight, log_sums, *rest):
    n, ntp = lax.axis_size("sp"), lax.axis_size("tp")
    rows, depth = latents.shape
    heads = rest[-1].shape[0]
    fits = heads * 2 == n and heads & (heads - 1) == 0 and heads > 1
    fits = fits and rows % 32 == 0 and BLOCK <= rows
    fits = fits and depth % (n * DV) == 0 and depth % (ntp * DV) == 0
    fits = fits and depth // ntp == value_weight.shape[1]
    run = by_level if fits else per_device
    return run(queries, key_vectors, latents, value_weight, log_sums, *rest)


def solution(mesh):
    return jax.shard_map(
        dispatch,
        mesh=mesh,
        in_specs=(
            P("sp", "tp"),
            P("sp", "tp"),
            P("sp", None),
            P(None, "tp"),
            P("sp", "tp"),
            P("sp", "tp"),
            P("sp", "tp"),
            P("sp", "tp"),
            P("tp"),
        ),
        out_specs=(P("sp", "tp"), P("sp", "tp"), P("sp", "tp"), P("sp", "tp")),
        check_vma=False,
    )
```

```python
import functools

import jax
import jax.numpy as jnp
from jax import lax
from jax.experimental import pallas as pl
from jax.experimental.pallas import tpu as pltpu
from jax.sharding import PartitionSpec as P

DH = 64
DV = 128
BLOCK = 256


def row_terms(out_first, out_second, cotangent, head_lambda):
    count = out_first.shape[0]
    head_count = head_lambda.shape[0]
    first = out_first.astype(jnp.float32).reshape(count, head_count, DV)
    second = out_second.astype(jnp.float32).reshape(count, head_count, DV)
    mixed = first - head_lambda[None, :, None] * second
    inverse = lax.rsqrt(jnp.mean(mixed * mixed, axis=-1, keepdims=True) + 1e-06)
    normed = mixed * inverse
    grad_out = cotangent.astype(jnp.float32).reshape(count, head_count, DV)
    grad_mixed = inverse * (grad_out - normed * jnp.mean(grad_out * normed, axis=-1, keepdims=True))
    grad_rows = grad_mixed.astype(jnp.bfloat16)
    widened = lax.optimization_barrier(grad_rows).astype(jnp.float32)
    row_dots = jnp.stack(
        [jnp.sum(widened * first, axis=-1), jnp.sum(widened * second, axis=-1)], axis=-1
    )
    return (grad_rows.reshape(count, head_count * DV), row_dots.reshape(count, head_count * 2))


def block_grads(
    query_rows, grad_rows, lse_rows, dot_rows, query_pos, key_rows, value_rows, key_pos, head_lambda
):
    count = query_rows.shape[0]
    width = key_rows.shape[0]
    head_count = head_lambda.shape[0]
    score_scale = DH ** (-0.5)
    query_heads = query_rows.reshape(count, head_count, 2, DH)
    key_heads = key_rows.reshape(width, head_count, 2, DH)
    grad_heads = grad_rows.reshape(count, head_count, DV)
    value_heads = value_rows.reshape(width, head_count, DV)
    scores = (
        jnp.einsum("nhad,mhad->hanm", query_heads, key_heads, preferred_element_type=jnp.float32)
        * score_scale
    )
    causal = query_pos[:, None] >= key_pos[None, :]
    shifts = lse_rows.reshape(count, head_count, 2).transpose(1, 2, 0)[..., None]
    probs = jnp.exp(jnp.where(causal, scores - shifts, -1e30))
    d_attn = jnp.einsum("nhe,mhe->hnm", grad_heads, value_heads, preferred_element_type=jnp.float32)
    dots = dot_rows.reshape(count, head_count, 2).transpose(1, 2, 0)[..., None]
    map_weight = jnp.stack([jnp.ones_like(head_lambda), -head_lambda], axis=1)[:, :, None, None]
    d_scores = (map_weight * probs * (d_attn[:, None] - dots)).astype(jnp.bfloat16)
    weights = (probs[:, 0] - head_lambda[:, None, None] * probs[:, 1]).astype(jnp.bfloat16)
    grad_q = (
        jnp.einsum("hanm,mhad->nhad", d_scores, key_heads, preferred_element_type=jnp.float32)
        * score_scale
    )
    grad_k = (
        jnp.einsum("hanm,nhad->mhad", d_scores, query_heads, preferred_element_type=jnp.float32)
        * score_scale
    )
    grad_v = jnp.einsum("hnm,nhe->mhe", weights, grad_heads, preferred_element_type=jnp.float32)
    return (grad_q.reshape(count, -1), grad_k.reshape(width, -1), grad_v.reshape(width, -1))


def per_device(
    queries,
    key_vectors,
    latents,
    value_weight,
    log_sums,
    out_first,
    out_second,
    cotangent,
    head_lambda,
):
    local_rows = queries.shape[0]
    offset = lax.axis_index("sp") * local_rows
    positions = offset + jnp.arange(local_rows, dtype=jnp.int32)
    last_row = offset + local_rows - 1
    values = jnp.dot(latents, value_weight, preferred_element_type=jnp.float32).astype(jnp.bfloat16)
    grad_rows, row_dots = row_terms(out_first, out_second, cotangent, head_lambda)
    gathered_stats = (
        lax.all_gather(log_sums, "sp", axis=0, tiled=True),
        lax.all_gather(row_dots, "sp", axis=0, tiled=True),
    )
    key_rows = lax.all_gather(key_vectors, "sp", axis=0, tiled=True)
    value_rows = lax.all_gather(values, "sp", axis=0, tiled=True)
    count = key_rows.shape[0]

    def compute(current):
        key_pos = jnp.arange(count, dtype=jnp.int32)
        grad_q, unused_k, unused_v = block_grads(
            queries,
            grad_rows,
            log_sums,
            row_dots,
            positions,
            key_rows,
            value_rows,
            key_pos,
            head_lambda,
        )
        return grad_q

    grad_queries = lax.cond(
        jnp.int32(0) <= last_row,
        compute,
        lambda current: current,
        jnp.zeros((local_rows, queries.shape[1]), jnp.float32),
    )
    start_totals = (
        jnp.zeros((local_rows, key_vectors.shape[1]), jnp.float32),
        jnp.zeros((local_rows, values.shape[1]), jnp.float32),
    )
    query_rows = lax.all_gather(queries, "sp", axis=0, tiled=True)
    grad_piece = lax.all_gather(grad_rows, "sp", axis=0, tiled=True)
    add_count = query_rows.shape[0]

    def compute(current):
        query_pos = jnp.arange(add_count, dtype=jnp.int32)
        lse_rows = gathered_stats[0]
        dot_rows = gathered_stats[1]
        unused_q, grad_k, grad_v = block_grads(
            query_rows,
            grad_piece,
            lse_rows,
            dot_rows,
            query_pos,
            key_vectors,
            values,
            positions,
            head_lambda,
        )
        return (grad_k, grad_v)

    grad_keys, grad_values = lax.cond(
        jnp.int32(0) + add_count - 1 >= offset, compute, lambda current: current, start_totals
    )
    values_grad = grad_values.astype(jnp.bfloat16)
    grad_weight = lax.psum_scatter(
        lax.dot_general(
            latents, values_grad, (((0,), (0,)), ((), ())), preferred_element_type=jnp.float32
        ).astype(jnp.bfloat16),
        "sp",
        scatter_dimension=0,
        tiled=True,
    ).astype(jnp.float32)
    latent_partial = lax.dot_general(
        values_grad, value_weight, (((1,), (1,)), ((), ())), preferred_element_type=jnp.float32
    )
    grad_latents = lax.psum_scatter(
        latent_partial.astype(jnp.bfloat16), "tp", scatter_dimension=1, tiled=True
    )
    return (grad_queries, grad_keys, grad_latents, grad_weight)


def level(z, k, nz):
    bit, out = 1, z
    while bit < nz:
        out = out + ((k // bit) % 2) * bit * (1 - 2 * ((z // bit) % 2))
        bit *= 2
    return out


def lanes(index, width=DV):
    return pl.ds(pl.multiple_of(index * width, width), width)


def chunk(index, rows):
    return pl.ds(pl.multiple_of(index * rows, rows), rows)


def remote(src, dst, send_sem, recv_sem, where):
    return pltpu.make_async_remote_copy(
        src_ref=src,
        dst_ref=dst,
        send_sem=send_sem,
        recv_sem=recv_sem,
        device_id=where,
        device_id_type=pl.DeviceIdType.MESH,
    )


def greet(devices):
    barrier = pltpu.get_barrier_semaphore()
    for device in devices:
        pl.semaphore_signal(
            barrier, inc=1, device_id=device, device_id_type=pl.DeviceIdType.MESH
        )
    return lambda: pl.semaphore_wait(barrier, len(devices))


NT = (((1,), (1,)), ((), ()))
TN = (((0,), (0,)), ((), ()))


def level_kernel(
    nz, ntp, q_ref, k_ref, lat_ref, w_ref, first_ref, second_ref, cot_ref, lse_ref, lambda_ref,
    q_home, k_home, gl_ref, gw_ref,
    first_s, second_s, cot_s, lat_s, w_s, grad_s, stat_s, v_s, q_all, do_all, k_all, v_all,
    stat_r, k0_s, k1_s, latp_s, qq_s, wide_s, dq_acc, dq_s, dkt_s, dvt_s, dk_s, dv_s,
    dko_s, dvo_s, dky_s, dvy_s, dks_s, dvs_s, v_pair, gl_s, gl_recv,
    up_send, up_recv, down_send, down_recv, sum_s,
    load_sem, own_sem, send_sem, recv_sem, pass_send, pass_recv, lat_send, lat_recv,
    q_send, q_recv, y_send, y_recv, z_send, z_recv, h_send, h_recv, t_send, t_recv,
    u_send, u_recv, d_send, d_recv
):
    sp, tp = lax.axis_index("sp"), lax.axis_index("tp")
    z, y = sp // 2, lax.rem(sp, 2)
    rows = q_ref.shape[0]
    width = latp_s.shape[2]
    partner = {"sp": 2 * z + 1 - y}
    peers = [{"sp": 2 * level(z, k, nz) + y} for k in range(1, nz)]
    bits = [1 << b for b in range(ntp.bit_length() - 1)]
    sides = {bit: {"tp": level(tp, bit, ntp)} for bit in bits}
    loads = [
        pltpu.make_async_copy(src, dst, load_sem.at[i])
        for i, (src, dst) in enumerate(
            [(lat_ref, lat_s), (w_ref, w_s), (first_ref, first_s), (second_ref, second_s),
             (cot_ref, cot_s)]
        )
    ]
    for load in loads:
        load.start()
    arrived = greet(peers + [partner] + list(sides.values()))
    own_q = pltpu.make_async_copy(q_ref.at[:, lanes(z)], q_all.at[z], own_sem.at[0])
    own_k = pltpu.make_async_copy(k_ref.at[:, lanes(z)], k_all.at[chunk(sp, rows)], own_sem.at[1])
    own_q.start()
    own_k.start()
    dkt_s[...] = jnp.zeros_like(dkt_s)
    dvt_s[...] = jnp.zeros_like(dvt_s)
    arrived()

    def send(part, k):
        to = level(z, k, nz)
        src, dst = {
            0: (q_ref.at[:, lanes(to)], q_all.at[z]),
            1: (grad_s.at[:, lanes(to)], do_all.at[z]),
            2: (stat_s.at[to], stat_r.at[z]),
            3: (k_ref.at[:, lanes(to)], k_all.at[chunk(sp, rows)]),
            4: (v_s.at[:, lanes(to)], v_all.at[chunk(sp, rows)]),
        }[part]
        return remote(src, dst, send_sem.at[part, k], recv_sem.at[part, k], peers[k - 1])

    def passed(part, k, own=None):
        kept = (k_all, v_all)[part]
        at = chunk(2 * level(z, k, nz) + y, rows)
        src = kept.at[at] if own is None else own
        return remote(src, kept.at[at], pass_send.at[part, k], pass_recv.at[part, k], partner)

    def lat_copy(t):
        return remote(
            lat_ref.at[:, lanes(2 * t + 1 - y, width)], latp_s.at[t],
            lat_send.at[t], lat_recv.at[t], partner
        )

    for k in range(1, nz):
        send(3, k).start()
    passed(0, 0, k_ref.at[:, lanes(z)]).start()
    for load in loads[:2]:
        load.wait()
    v_s[...] = jnp.dot(lat_s[...], w_s[...], preferred_element_type=jnp.float32).astype(
        jnp.bfloat16
    )
    for k in range(1, nz):
        send(4, k).start()
    passed(1, 0, v_s.at[:, lanes(z)]).start()
    own_v = pltpu.make_async_copy(v_s.at[:, lanes(z)], v_all.at[chunk(sp, rows)], own_sem.at[2])
    own_v.start()
    for load in loads[2:]:
        load.wait()
    columns = []
    for head in range(nz):
        at = slice(head * DV, (head + 1) * DV)
        first = first_s[:, at].astype(jnp.float32)
        second = second_s[:, at].astype(jnp.float32)
        mixed = first - lambda_ref[head] * second
        inverse = lax.rsqrt(jnp.mean(mixed * mixed, axis=-1, keepdims=True) + 1e-06)
        normed = mixed * inverse
        grad_out = cot_s[:, at].astype(jnp.float32)
        mean_dot = jnp.mean(grad_out * normed, axis=-1, keepdims=True)
        grad_rows = (inverse * (grad_out - normed * mean_dot)).astype(jnp.bfloat16)
        grad_s[:, at] = grad_rows
        widened = grad_rows.astype(jnp.float32)
        columns.append(jnp.sum(widened * first, axis=-1, keepdims=True))
        columns.append(jnp.sum(widened * second, axis=-1, keepdims=True))
    dots = jnp.concatenate(columns, axis=1).T
    for head in range(nz):
        pair = slice(2 * head, 2 * head + 2)
        stat_s[head] = jnp.concatenate(
            [lse_ref[pair, :], dots[pair, :], jnp.zeros((4, rows), jnp.float32)], axis=0
        )
    for k in range(1, nz):
        for part in (2, 0, 1):
            send(part, k).start()
    own_do = pltpu.make_async_copy(grad_s.at[:, lanes(z)], do_all.at[z], own_sem.at[3])
    own_do.start()
    stat_r[z] = stat_s[z]

    for part in (3, 4):
        for k in range(1, nz):
            send(part, k).wait_recv()
            passed(part - 3, k).start()
    for t in range(nz):
        lat_copy(t).start()
    own_k.wait()
    own_v.wait()
    for part in range(2):
        for k in range(nz):
            passed(part, k).wait_recv()
    keys = k_all[...]
    half = lax.broadcasted_iota(jnp.int32, keys.shape, 1) < DH
    k0_s[...] = jnp.where(half, keys, jnp.zeros_like(keys))
    k1_s[...] = jnp.where(half, jnp.zeros_like(keys), keys)
    weight = lambda_ref[z]
    scale = jnp.bfloat16(DH**-0.5)

    def q_copy(k):
        return remote(
            dq_s.at[k], q_home.at[:, lanes(z)], q_send.at[k], q_recv.at[k], peers[k - 1]
        )

    for k in range(nz):
        at = level(z, k, nz)
        if k == 0:
            own_q.wait()
            own_do.wait()
        else:
            for part in range(3):
                send(part, k).wait_recv()
        queries = q_all[at] * scale
        left = lax.broadcasted_iota(jnp.int32, queries.shape, 1) < DH
        qq_s[0:rows, :] = jnp.where(left, queries, jnp.zeros_like(queries))
        qq_s[rows:, :] = jnp.where(left, jnp.zeros_like(queries), queries)
        queries_t = queries.T
        grads_t = do_all[at].T
        stats = stat_r[at].T
        for i in range(4):
            wide_s[i] = jnp.broadcast_to(stats[:, i : i + 1], (rows, BLOCK))
        dq_acc[...] = jnp.zeros_like(dq_acc)
        place = 2 * at + y
        full = (place * rows + 1) // BLOCK
        end = ((place + 1) * rows - 1) // BLOCK + 1

        def tile(t, masked):
            key_rows = chunk(t, BLOCK)
            s01 = lax.dot_general(
                qq_s[...], k_all[key_rows, :], NT, preferred_element_type=jnp.float32
            )
            d_attn = lax.dot_general(
                do_all[at], v_all[key_rows, :], NT, preferred_element_type=jnp.float32
            )
            x0 = s01[:rows] - wide_s[0]
            x1 = s01[rows:] - wide_s[1]
            if masked:
                key_at = lax.broadcasted_iota(jnp.int32, (rows, BLOCK), 1) + t * BLOCK
                query_at = lax.broadcasted_iota(jnp.int32, (rows, BLOCK), 0) + place * rows
                x0 = jnp.where(key_at <= query_at, x0, -1e30)
                x1 = jnp.where(key_at <= query_at, x1, -1e30)
            p0 = jnp.exp(x0)
            p1 = weight * jnp.exp(x1)
            ds0 = (p0 * (d_attn - wide_s[2])).astype(jnp.bfloat16)
            ds1 = (p1 * (wide_s[3] - d_attn)).astype(jnp.bfloat16)
            w = (p0 - p1).astype(jnp.bfloat16)
            dq_acc[...] += jnp.dot(
                ds0, k0_s[key_rows, :], preferred_element_type=jnp.float32
            ) + jnp.dot(ds1, k1_s[key_rows, :], preferred_element_type=jnp.float32)
            columns = lanes(t, BLOCK)
            dkt_s[:DH, columns] += jnp.dot(
                queries_t[:DH], ds0, preferred_element_type=jnp.float32
            )
            dkt_s[DH:, columns] += jnp.dot(
                queries_t[DH:], ds1, preferred_element_type=jnp.float32
            )
            dvt_s[:, columns] += jnp.dot(grads_t, w, preferred_element_type=jnp.float32)

        def full_tiles(t, carry):
            tile(t, False)
            return carry

        def edge_tiles(t, carry):
            tile(t, True)
            return carry

        lax.fori_loop(0, full, full_tiles, 0)
        lax.fori_loop(full, end, edge_tiles, 0)
        grad_q = (dq_acc[...] * DH ** (-0.5)).astype(jnp.bfloat16)
        if k == 0:
            q_home[:, lanes(z)] = grad_q
        else:
            dq_s[k] = grad_q
            q_copy(k).start()

    def y_copy(part, k):
        at = level(z, k, nz)
        src, dst = ((dvo_s, dvy_s), (dko_s, dky_s))[part]
        return remote(src.at[at], dst.at[at], y_send.at[part, k], y_recv.at[part, k], partner)

    def z_copy(part, k):
        at = level(z, k, nz)
        src = (dvs_s, dks_s)[part].at[at]
        dst = v_pair.at[0:rows, lanes(z)] if part == 0 else k_home.at[:, lanes(z)]
        return remote(src, dst, z_send.at[part, k], z_recv.at[part, k], peers[k - 1])

    def home_copy(k):
        head = level(z, k, nz)
        return remote(
            v_pair.at[0:rows, lanes(head)], v_pair.at[rows : 2 * rows, lanes(head)],
            h_send.at[k], h_recv.at[k], partner
        )

    order = list(range(1, nz)) + [0]
    for part, (turned, flat, other) in enumerate(((dvt_s, dv_s, dvo_s), (dkt_s, dk_s, dko_s))):
        for t in range(flat.shape[0] // BLOCK):
            at = slice(t * BLOCK, (t + 1) * BLOCK)
            flat[at, :] = turned[:, at].T
        for k in order:
            at = level(z, k, nz)
            other[at] = flat[chunk(2 * at + 1 - y, rows), :].astype(jnp.bfloat16)
            y_copy(part, k).start()
    for part, (flat, got, total) in enumerate(((dv_s, dvy_s, dvs_s), (dk_s, dky_s, dks_s))):
        for k in order:
            at = level(z, k, nz)
            y_copy(part, k).wait_recv()
            added = flat[chunk(2 * at + y, rows), :] + got[at].astype(jnp.float32)
            added = added.astype(jnp.bfloat16)
            if k == 0:
                if part == 0:
                    v_pair[0:rows, lanes(z)] = added
                else:
                    k_home[:, lanes(z)] = added
            else:
                total[at] = added
                z_copy(part, k).start()
    home_copy(0).start()
    for k in range(1, nz):
        z_copy(0, k).wait_recv()
        home_copy(k).start()

    own_rows = v_pair[0:rows, :]
    share = gl_ref.shape[1]

    def latent_term(o):
        at = chunk(level(tp, o, ntp), share)
        return lax.dot_general(
            own_rows, w_s[at, :], NT, preferred_element_type=jnp.float32
        ).astype(jnp.bfloat16)

    def side_copy(bit, o):
        return remote(
            gl_s.at[o], gl_recv.at[o], t_send.at[o], t_recv.at[o], sides[bit]
        )

    alive = list(range(ntp))
    moves = []
    for bit in bits:
        leaving = [o for o in alive if o & bit]
        if bit == 1:
            for o in leaving:
                gl_s[o] = latent_term(o)
                side_copy(bit, o).start()
            alive = [o for o in alive if not o & bit]
            for o in alive:
                gl_s[o] = latent_term(o)
        else:
            for o in leaving:
                side_copy(bit, o).start()
            alive = [o for o in alive if not o & bit]
        moves.append((bit, leaving, alive))
        if bit != bits[-1]:
            for o in leaving:
                side_copy(bit, o).wait_recv()
            for o in alive:
                gl_s[o] = (
                    gl_s[o].astype(jnp.float32) + gl_recv[o + bit].astype(jnp.float32)
                ).astype(jnp.bfloat16)
    for t in range(nz):
        lat_copy(t).wait_recv()
    for k in range(nz):
        home_copy(k).wait_recv()

    parts = up_send.shape[1]
    piece = width // parts

    def term(t, s):
        at = pl.ds(pl.multiple_of((2 * t + y) * width + s * piece, piece), piece)
        own = lat_s[:, at]
        other = latp_s[t, :, s * piece : (s + 1) * piece]
        return lax.dot_general(
            jnp.concatenate([own, other], axis=0), v_pair[...], TN,
            preferred_element_type=jnp.float32,
        )

    def line_copy(up, t, s):
        if up:
            return remote(
                up_send.at[t, s], up_recv.at[t, s], u_send.at[t, s], u_recv.at[t, s],
                {"sp": 2 * (z + 1) + y}
            )
        return remote(
            down_send.at[t, s], down_recv.at[t, s], d_send.at[t, s], d_recv.at[t, s],
            {"sp": 2 * (z - 1) + y}
        )

    hops = []
    for i in range(nz - 1):
        hops += [(True, nz - 1 - i), (False, i)]

    for up, t in hops:
        for s in range(parts):
            @pl.when((z < t) if up else (z > t))
            def _():
                sum_s[...] = term(t, s)

                @pl.when((z > 0) if up else (z < nz - 1))
                def _():
                    line_copy(up, t, s).wait_recv()
                    sum_s[...] += (up_recv if up else down_recv)[t, s].astype(jnp.float32)

                (up_send if up else down_send)[t, s] = sum_s[...].astype(jnp.bfloat16)
                line_copy(up, t, s).start()

    last = bits[-1]
    side_copy(last, last).wait_recv()
    gl_ref[...] = (gl_s[0].astype(jnp.float32) + gl_recv[last].astype(jnp.float32)).astype(
        jnp.bfloat16
    )
    for s in range(parts):
        at = slice(s * piece, (s + 1) * piece)
        gw_ref[at, :] = term(z, s)
    for k in range(1, nz):
        q_copy(k).wait_recv()
        z_copy(1, k).wait_recv()
    for t in range(nz):
        for s in range(parts):
            at = slice(s * piece, (s + 1) * piece)
            if t > 0:
                @pl.when(z == t)
                def _():
                    line_copy(True, t, s).wait_recv()
                    gw_ref[at, :] += up_recv[t, s].astype(jnp.float32)
            if t < nz - 1:
                @pl.when(z == t)
                def _():
                    line_copy(False, t, s).wait_recv()
                    gw_ref[at, :] += down_recv[t, s].astype(jnp.float32)
    for up, t in hops:
        for s in range(parts):
            @pl.when((z < t) if up else (z > t))
            def _():
                line_copy(up, t, s).wait_send()
    for k in range(1, nz):
        for part in range(5):
            send(part, k).wait_send()
        q_copy(k).wait_send()
        for part in range(2):
            z_copy(part, k).wait_send()
    for k in range(nz):
        lat_copy(k).wait_send()
        home_copy(k).wait_send()
        for part in range(2):
            passed(part, k).wait_send()
            y_copy(part, k).wait_send()
    for bit, leaving, _ in moves:
        for o in leaving:
            side_copy(bit, o).wait_send()


def level_call(
    queries, keys, latents, value_weight, first, second, cotangent, lse, head_lambda, n, ntp
):
    rows = queries.shape[0]
    depth, wide = value_weight.shape
    nz = n // 2
    width, share = depth // n, depth // ntp
    parts = 2 if width % 256 == 0 else 1
    dense, exact = jnp.bfloat16, jnp.float32
    vmem = pl.BlockSpec(memory_space=pltpu.VMEM)
    hbm = pl.BlockSpec(memory_space=pl.ANY)
    sem = pltpu.SemaphoreType.DMA
    buffers = (
        [((rows, wide), dense)] * 3
        + [((rows, depth), dense), ((depth, wide), dense)]
        + [((rows, wide), dense), ((nz, 8, rows), exact), ((rows, wide), dense)]
        + [((nz, rows, DV), dense)] * 2
        + [((n * rows, DV), dense)] * 2
        + [((nz, 8, rows), exact)]
        + [((n * rows, DV), dense)] * 2
        + [((nz, rows, width), dense), ((2 * rows, DV), dense), ((4, rows, BLOCK), exact)]
        + [((rows, DV), exact), ((nz, rows, DV), dense)]
        + [((DV, n * rows), exact)] * 2
        + [((n * rows, DV), exact)] * 2
        + [((nz, rows, DV), dense)] * 6
        + [((2 * rows, wide), dense)]
        + [((ntp, rows, share), dense)] * 2
        + [((nz, parts, width // parts, wide), dense)] * 4
        + [((width // parts, wide), exact)]
    )
    sems = (
        [(5,), (4,), (5, nz), (5, nz), (2, nz), (2, nz), (nz,), (nz,)]
        + [(nz,), (nz,), (2, nz), (2, nz), (2, nz), (2, nz), (nz,), (nz,), (ntp,), (ntp,)]
        + [(nz, parts)] * 4
    )
    return pl.pallas_call(
        functools.partial(level_kernel, nz, ntp),
        out_shape=[
            jax.ShapeDtypeStruct((rows, wide), dense),
            jax.ShapeDtypeStruct((rows, wide), dense),
            jax.ShapeDtypeStruct((rows, share), dense),
            jax.ShapeDtypeStruct((width, wide), exact),
        ],
        in_specs=[hbm] * 7 + [vmem, pl.BlockSpec(memory_space=pltpu.SMEM)],
        out_specs=[vmem] * 4,
        scratch_shapes=[pltpu.VMEM(*b) for b in buffers] + [sem(s) for s in sems],
        compiler_params=pltpu.CompilerParams(collective_id=1, has_side_effects=True),
    )(queries, keys, latents, value_weight, first, second, cotangent, lse, head_lambda)


def finish_kernel(q_ref, k_ref, gl_ref, gw_ref, q_out, k_out, gl_out, gw_out):
    q_out[...] = q_ref[...].astype(jnp.float32)
    k_out[...] = k_ref[...].astype(jnp.float32)
    gl_out[...] = gl_ref[...]
    gw_out[...] = gw_ref[...]


def finish(q_home, k_home, gl, gw):
    vmem = pl.BlockSpec(memory_space=pltpu.VMEM)
    kinds = ((q_home, jnp.float32), (k_home, jnp.float32), (gl, gl.dtype), (gw, gw.dtype))
    return pl.pallas_call(
        finish_kernel,
        out_shape=[jax.ShapeDtypeStruct(a.shape, kind) for a, kind in kinds],
        in_specs=[vmem] * 4,
        out_specs=[vmem] * 4,
    )(q_home, k_home, gl, gw)


def by_level(
    queries, key_vectors, latents, value_weight, log_sums, out_first, out_second, cotangent,
    head_lambda
):
    n, ntp = lax.axis_size("sp"), lax.axis_size("tp")
    return tuple(
        finish(
            *level_call(
                queries, key_vectors, latents, value_weight, out_first, out_second, cotangent,
                log_sums.T, head_lambda, n, ntp
            )
        )
    )


def dispatch(queries, key_vectors, latents, value_weight, log_sums, *rest):
    n, ntp = lax.axis_size("sp"), lax.axis_size("tp")
    rows, depth = latents.shape
    heads = rest[-1].shape[0]
    fits = heads * 2 == n and heads & (heads - 1) == 0 and heads > 1
    fits = fits and ntp & (ntp - 1) == 0 and ntp > 1
    fits = fits and rows % 32 == 0 and (n * rows) % BLOCK == 0
    fits = fits and depth % (n * DV) == 0 and depth % (ntp * DV) == 0
    fits = fits and depth // ntp == value_weight.shape[1]
    run = by_level if fits else per_device
    return run(queries, key_vectors, latents, value_weight, log_sums, *rest)


def solution(mesh):
    return jax.shard_map(
        dispatch,
        mesh=mesh,
        in_specs=(
            P("sp", "tp"),
            P("sp", "tp"),
            P("sp", None),
            P(None, "tp"),
            P("sp", "tp"),
            P("sp", "tp"),
            P("sp", "tp"),
            P("sp", "tp"),
            P("tp"),
        ),
        out_specs=(P("sp", "tp"), P("sp", "tp"), P("sp", "tp"), P("sp", "tp")),
        check_vma=False,
    )
```

```python
import functools

import jax
import jax.numpy as jnp
from jax import lax
from jax.experimental import pallas as pl
from jax.experimental.pallas import tpu as pltpu
from jax.sharding import PartitionSpec as P

DH = 64
DV = 128
BLOCK = 256


def row_terms(out_first, out_second, cotangent, head_lambda):
    count = out_first.shape[0]
    head_count = head_lambda.shape[0]
    first = out_first.astype(jnp.float32).reshape(count, head_count, DV)
    second = out_second.astype(jnp.float32).reshape(count, head_count, DV)
    mixed = first - head_lambda[None, :, None] * second
    inverse = lax.rsqrt(jnp.mean(mixed * mixed, axis=-1, keepdims=True) + 1e-06)
    normed = mixed * inverse
    grad_out = cotangent.astype(jnp.float32).reshape(count, head_count, DV)
    grad_mixed = inverse * (grad_out - normed * jnp.mean(grad_out * normed, axis=-1, keepdims=True))
    grad_rows = grad_mixed.astype(jnp.bfloat16)
    widened = lax.optimization_barrier(grad_rows).astype(jnp.float32)
    row_dots = jnp.stack(
        [jnp.sum(widened * first, axis=-1), jnp.sum(widened * second, axis=-1)], axis=-1
    )
    return (grad_rows.reshape(count, head_count * DV), row_dots.reshape(count, head_count * 2))


def block_grads(
    query_rows, grad_rows, lse_rows, dot_rows, query_pos, key_rows, value_rows, key_pos, head_lambda
):
    count = query_rows.shape[0]
    width = key_rows.shape[0]
    head_count = head_lambda.shape[0]
    score_scale = DH ** (-0.5)
    query_heads = query_rows.reshape(count, head_count, 2, DH)
    key_heads = key_rows.reshape(width, head_count, 2, DH)
    grad_heads = grad_rows.reshape(count, head_count, DV)
    value_heads = value_rows.reshape(width, head_count, DV)
    scores = (
        jnp.einsum("nhad,mhad->hanm", query_heads, key_heads, preferred_element_type=jnp.float32)
        * score_scale
    )
    causal = query_pos[:, None] >= key_pos[None, :]
    shifts = lse_rows.reshape(count, head_count, 2).transpose(1, 2, 0)[..., None]
    probs = jnp.exp(jnp.where(causal, scores - shifts, -1e30))
    d_attn = jnp.einsum("nhe,mhe->hnm", grad_heads, value_heads, preferred_element_type=jnp.float32)
    dots = dot_rows.reshape(count, head_count, 2).transpose(1, 2, 0)[..., None]
    map_weight = jnp.stack([jnp.ones_like(head_lambda), -head_lambda], axis=1)[:, :, None, None]
    d_scores = (map_weight * probs * (d_attn[:, None] - dots)).astype(jnp.bfloat16)
    weights = (probs[:, 0] - head_lambda[:, None, None] * probs[:, 1]).astype(jnp.bfloat16)
    grad_q = (
        jnp.einsum("hanm,mhad->nhad", d_scores, key_heads, preferred_element_type=jnp.float32)
        * score_scale
    )
    grad_k = (
        jnp.einsum("hanm,nhad->mhad", d_scores, query_heads, preferred_element_type=jnp.float32)
        * score_scale
    )
    grad_v = jnp.einsum("hnm,nhe->mhe", weights, grad_heads, preferred_element_type=jnp.float32)
    return (grad_q.reshape(count, -1), grad_k.reshape(width, -1), grad_v.reshape(width, -1))


def per_device(
    queries,
    key_vectors,
    latents,
    value_weight,
    log_sums,
    out_first,
    out_second,
    cotangent,
    head_lambda,
):
    local_rows = queries.shape[0]
    offset = lax.axis_index("sp") * local_rows
    positions = offset + jnp.arange(local_rows, dtype=jnp.int32)
    last_row = offset + local_rows - 1
    values = jnp.dot(latents, value_weight, preferred_element_type=jnp.float32).astype(jnp.bfloat16)
    grad_rows, row_dots = row_terms(out_first, out_second, cotangent, head_lambda)
    gathered_stats = (
        lax.all_gather(log_sums, "sp", axis=0, tiled=True),
        lax.all_gather(row_dots, "sp", axis=0, tiled=True),
    )
    key_rows = lax.all_gather(key_vectors, "sp", axis=0, tiled=True)
    value_rows = lax.all_gather(values, "sp", axis=0, tiled=True)
    count = key_rows.shape[0]

    def compute(current):
        key_pos = jnp.arange(count, dtype=jnp.int32)
        grad_q, unused_k, unused_v = block_grads(
            queries,
            grad_rows,
            log_sums,
            row_dots,
            positions,
            key_rows,
            value_rows,
            key_pos,
            head_lambda,
        )
        return grad_q

    grad_queries = lax.cond(
        jnp.int32(0) <= last_row,
        compute,
        lambda current: current,
        jnp.zeros((local_rows, queries.shape[1]), jnp.float32),
    )
    start_totals = (
        jnp.zeros((local_rows, key_vectors.shape[1]), jnp.float32),
        jnp.zeros((local_rows, values.shape[1]), jnp.float32),
    )
    query_rows = lax.all_gather(queries, "sp", axis=0, tiled=True)
    grad_piece = lax.all_gather(grad_rows, "sp", axis=0, tiled=True)
    add_count = query_rows.shape[0]

    def compute(current):
        query_pos = jnp.arange(add_count, dtype=jnp.int32)
        lse_rows = gathered_stats[0]
        dot_rows = gathered_stats[1]
        unused_q, grad_k, grad_v = block_grads(
            query_rows,
            grad_piece,
            lse_rows,
            dot_rows,
            query_pos,
            key_vectors,
            values,
            positions,
            head_lambda,
        )
        return (grad_k, grad_v)

    grad_keys, grad_values = lax.cond(
        jnp.int32(0) + add_count - 1 >= offset, compute, lambda current: current, start_totals
    )
    values_grad = grad_values.astype(jnp.bfloat16)
    grad_weight = lax.psum_scatter(
        lax.dot_general(
            latents, values_grad, (((0,), (0,)), ((), ())), preferred_element_type=jnp.float32
        ).astype(jnp.bfloat16),
        "sp",
        scatter_dimension=0,
        tiled=True,
    ).astype(jnp.float32)
    latent_partial = lax.dot_general(
        values_grad, value_weight, (((1,), (1,)), ((), ())), preferred_element_type=jnp.float32
    )
    grad_latents = lax.psum_scatter(
        latent_partial.astype(jnp.bfloat16), "tp", scatter_dimension=1, tiled=True
    )
    return (grad_queries, grad_keys, grad_latents, grad_weight)


def level(z, k, nz):
    bit, out = 1, z
    while bit < nz:
        out = out + ((k // bit) % 2) * bit * (1 - 2 * ((z // bit) % 2))
        bit *= 2
    return out


def lanes(index, width=DV):
    return pl.ds(pl.multiple_of(index * width, width), width)


def chunk(index, rows):
    return pl.ds(pl.multiple_of(index * rows, rows), rows)


def remote(src, dst, send_sem, recv_sem, where):
    return pltpu.make_async_remote_copy(
        src_ref=src,
        dst_ref=dst,
        send_sem=send_sem,
        recv_sem=recv_sem,
        device_id=where,
        device_id_type=pl.DeviceIdType.MESH,
    )


def greet(devices):
    barrier = pltpu.get_barrier_semaphore()
    for device in devices:
        pl.semaphore_signal(
            barrier, inc=1, device_id=device, device_id_type=pl.DeviceIdType.MESH
        )
    return lambda: pl.semaphore_wait(barrier, len(devices))


NT = (((1,), (1,)), ((), ()))
TN = (((0,), (0,)), ((), ()))


def level_kernel(
    nz, ntp, q_ref, k_ref, lat_ref, w_ref, first_ref, second_ref, cot_ref, lse_ref, lambda_ref,
    q_home, k_home, gl_ref, gw_ref,
    first_s, second_s, cot_s, lat_s, w_s, grad_s, stat_s, v_s, q_all, do_all, k_all, v_all,
    stat_r, stat_t, q0_s, q1_s, latp_s, kk_s, s0_s, s1_s, a0_s, a1_s, dk_acc, dv_acc, dqt_s, dq_s,
    dqo_s, dqy_s, dqs_s, dks_s, dvs_s, v_pair, gl_s, gl_recv,
    line_send, line_recv, sum_s,
    load_sem, own_sem, send_sem, recv_sem, pass_send, pass_recv, lat_send, lat_recv,
    y_send, y_recv, z_send, z_recv, h_send, h_recv, t_send, t_recv,
    u_send, u_recv
):
    sp, tp = lax.axis_index("sp"), lax.axis_index("tp")
    z, y = sp // 2, lax.rem(sp, 2)
    rows = q_ref.shape[0]
    width = latp_s.shape[2]
    partner = {"sp": 2 * z + 1 - y}
    peers = [{"sp": 2 * level(z, k, nz) + y} for k in range(1, nz)]
    bits = [1 << b for b in range(ntp.bit_length() - 1)]
    sides = {bit: {"tp": level(tp, bit, ntp)} for bit in bits}
    loads = [
        pltpu.make_async_copy(src, dst, load_sem.at[i])
        for i, (src, dst) in enumerate(
            [(first_ref, first_s), (second_ref, second_s), (cot_ref, cot_s), (lat_ref, lat_s),
             (w_ref, w_s)]
        )
    ]
    for load in loads:
        load.start()
    arrived = greet(peers + [partner] + list(sides.values()))
    own_q = pltpu.make_async_copy(
        q_ref.at[:, lanes(z)], q_all.at[chunk(sp, rows)], own_sem.at[0]
    )
    own_k = pltpu.make_async_copy(k_ref.at[:, lanes(z)], k_all.at[z], own_sem.at[1])
    own_q.start()
    own_k.start()
    dqt_s[...] = jnp.zeros_like(dqt_s)
    arrived()

    def send(part, k):
        to = level(z, k, nz)
        src, dst = {
            0: (q_ref.at[:, lanes(to)], q_all.at[chunk(sp, rows)]),
            1: (grad_s.at[:, lanes(to)], do_all.at[chunk(sp, rows)]),
            2: (stat_s.at[to], stat_r.at[sp]),
            3: (k_ref.at[:, lanes(to)], k_all.at[z]),
            4: (v_s.at[:, lanes(to)], v_all.at[z]),
        }[part]
        return remote(src, dst, send_sem.at[part, k], recv_sem.at[part, k], peers[k - 1])

    def passed(part, k, own=None):
        at = 2 * level(z, k, nz) + y
        kept = (q_all, do_all, stat_r)[part].at[at if part == 2 else chunk(at, rows)]
        src = kept if own is None else own
        return remote(src, kept, pass_send.at[part, k], pass_recv.at[part, k], partner)

    def lat_copy(t):
        return remote(
            lat_ref.at[:, lanes(2 * t + 1 - y, width)], latp_s.at[t],
            lat_send.at[t], lat_recv.at[t], partner
        )

    for k in range(1, nz):
        send(0, k).start()
    passed(0, 0, q_ref.at[:, lanes(z)]).start()
    for load in loads[:3]:
        load.wait()
    columns = []
    for head in range(nz):
        at = slice(head * DV, (head + 1) * DV)
        first = first_s[:, at].astype(jnp.float32)
        second = second_s[:, at].astype(jnp.float32)
        mixed = first - lambda_ref[head] * second
        inverse = lax.rsqrt(jnp.mean(mixed * mixed, axis=-1, keepdims=True) + 1e-06)
        normed = mixed * inverse
        grad_out = cot_s[:, at].astype(jnp.float32)
        mean_dot = jnp.mean(grad_out * normed, axis=-1, keepdims=True)
        grad_rows = (inverse * (grad_out - normed * mean_dot)).astype(jnp.bfloat16)
        grad_s[:, at] = grad_rows
        widened = grad_rows.astype(jnp.float32)
        columns.append(jnp.sum(widened * first, axis=-1, keepdims=True))
        columns.append(jnp.sum(widened * second, axis=-1, keepdims=True))
    dots = jnp.concatenate(columns, axis=1).T
    for head in range(nz):
        pair = slice(2 * head, 2 * head + 2)
        stat_s[head] = jnp.concatenate(
            [lse_ref[pair, :], dots[pair, :], jnp.zeros((4, rows), jnp.float32)], axis=0
        )
    for k in range(1, nz):
        for part in (2, 1):
            send(part, k).start()
    passed(2, 0, stat_s.at[z]).start()
    passed(1, 0, grad_s.at[:, lanes(z)]).start()
    own_do = pltpu.make_async_copy(
        grad_s.at[:, lanes(z)], do_all.at[chunk(sp, rows)], own_sem.at[2]
    )
    own_do.start()
    stat_r[sp] = stat_s[z]
    for load in loads[3:]:
        load.wait()
    v_s[...] = jnp.dot(lat_s[...], w_s[...], preferred_element_type=jnp.float32).astype(
        jnp.bfloat16
    )
    for k in range(1, nz):
        for part in (3, 4):
            send(part, k).start()
    own_v = pltpu.make_async_copy(v_s.at[:, lanes(z)], v_all.at[z], own_sem.at[3])
    own_v.start()
    for part in (0, 2, 1):
        for k in range(1, nz):
            send(part, k).wait_recv()
            passed(part, k).start()
    for t in range(nz):
        lat_copy(t).start()
    own_q.wait()
    own_do.wait()
    for part in range(3):
        for k in range(nz):
            passed(part, k).wait_recv()
    scale = jnp.bfloat16(DH**-0.5)
    queries = q_all[...] * scale
    half = lax.broadcasted_iota(jnp.int32, queries.shape, 1) < DH
    q0_s[...] = jnp.where(half, queries, jnp.zeros_like(queries))
    q1_s[...] = jnp.where(half, jnp.zeros_like(queries), queries)
    tiles = stat_t.shape[0]
    stats = jnp.concatenate([stat_r[c] for c in range(2 * nz)], axis=1)
    for t in range(tiles):
        stat_t[t] = stats[:, t * BLOCK : (t + 1) * BLOCK]
    weight = lambda_ref[z]

    def z_copy(part, k):
        src = (dvs_s, dks_s, dqs_s)[part].at[k]
        dst = (
            v_pair.at[0:rows, lanes(z)], k_home.at[:, lanes(z)], q_home.at[:, lanes(z)]
        )[part]
        return remote(src, dst, z_send.at[part, k], z_recv.at[part, k], peers[k - 1])

    def home_copy(k):
        head = level(z, k, nz)
        return remote(
            v_pair.at[0:rows, lanes(head)], v_pair.at[rows : 2 * rows, lanes(head)],
            h_send.at[k], h_recv.at[k], partner
        )

    for k in range(nz):
        at = level(z, k, nz)
        if k == 0:
            own_k.wait()
            own_v.wait()
        else:
            for part in (3, 4):
                send(part, k).wait_recv()
        keys = k_all[at]
        keys_t = keys.T
        keys = keys * scale
        left = lax.broadcasted_iota(jnp.int32, keys.shape, 1) < DH
        kk_s[0:rows, :] = jnp.where(left, keys, jnp.zeros_like(keys))
        kk_s[rows:, :] = jnp.where(left, jnp.zeros_like(keys), keys)
        dk_acc[...] = jnp.zeros_like(dk_acc)
        dv_acc[...] = jnp.zeros_like(dv_acc)
        place = 2 * at + y
        begin = (place * rows) // BLOCK

        def scores(t, held):
            query_rows = chunk(t, BLOCK)
            held[0][...] = lax.dot_general(
                kk_s[...], q_all[query_rows, :], NT, preferred_element_type=jnp.float32
            )
            held[1][...] = lax.dot_general(
                v_all[at], do_all[query_rows, :], NT, preferred_element_type=jnp.float32
            )

        def tile(t, held):
            query_rows = chunk(t, BLOCK)
            stat = stat_t[t]
            d_attn = held[1][...]
            key_at = lax.broadcasted_iota(jnp.int32, (rows, BLOCK), 0)
            query_at = lax.broadcasted_iota(jnp.int32, (rows, BLOCK), 1)
            seen = key_at - query_at <= t * BLOCK - place * rows
            p0 = jnp.exp(jnp.where(seen, held[0][:rows, :] - stat[0:1, :], -1e30))
            p1 = weight * jnp.exp(jnp.where(seen, held[0][rows:, :] - stat[1:2, :], -1e30))
            ds0 = (p0 * (d_attn - stat[2:3, :])).astype(jnp.bfloat16)
            ds1 = (p1 * (stat[3:4, :] - d_attn)).astype(jnp.bfloat16)
            w = (p0 - p1).astype(jnp.bfloat16)
            dk_acc[...] += jnp.dot(
                ds0, q0_s[query_rows, :], preferred_element_type=jnp.float32
            ) + jnp.dot(ds1, q1_s[query_rows, :], preferred_element_type=jnp.float32)
            dv_acc[...] += jnp.dot(w, do_all[query_rows, :], preferred_element_type=jnp.float32)
            columns = lanes(t, BLOCK)
            dqt_s[:DH, columns] += jnp.dot(keys_t[:DH], ds0, preferred_element_type=jnp.float32)
            dqt_s[DH:, columns] += jnp.dot(keys_t[DH:], ds1, preferred_element_type=jnp.float32)

        even, odd = (s0_s, a0_s), (s1_s, a1_s)
        scores(begin, even)

        def pair(i, carry):
            t = begin + 2 * i
            scores(t + 1, odd)
            tile(t, even)
            scores(jnp.minimum(t + 2, tiles - 1), even)
            tile(t + 1, odd)
            return carry

        lax.fori_loop(0, (tiles - begin) // 2, pair, 0)

        @pl.when((tiles - begin) % 2 == 1)
        def _():
            tile(tiles - 1, even)

        grad_v, grad_k = dv_acc[...].astype(jnp.bfloat16), dk_acc[...].astype(jnp.bfloat16)
        if k == 0:
            v_pair[0:rows, lanes(z)] = grad_v
            k_home[:, lanes(z)] = grad_k
            home_copy(0).start()
        else:
            dvs_s[k] = grad_v
            z_copy(0, k).start()
            dks_s[k] = grad_k
            z_copy(1, k).start()

    def y_copy(k):
        at = level(z, k, nz)
        return remote(dqo_s.at[at], dqy_s.at[at], y_send.at[k], y_recv.at[k], partner)

    order = list(range(1, nz)) + [0]
    for t in range(tiles):
        at = slice(t * BLOCK, (t + 1) * BLOCK)
        dq_s[at, :] = (dqt_s[:, at] * DH ** (-0.5)).T
    for k in order:
        at = level(z, k, nz)
        dqo_s[at] = dq_s[chunk(2 * at + 1 - y, rows), :].astype(jnp.bfloat16)
        y_copy(k).start()
    for k in range(1, nz - 1):
        z_copy(0, k).wait_recv()
        home_copy(k).start()
    for k in order:
        at = level(z, k, nz)
        y_copy(k).wait_recv()
        added = dq_s[chunk(2 * at + y, rows), :] + dqy_s[at].astype(jnp.float32)
        if k == 0:
            q_home[:, lanes(z)] = added.astype(jnp.bfloat16)
        else:
            dqs_s[k] = added.astype(jnp.bfloat16)
            z_copy(2, k).start()
    for k in range(nz - 1, nz):
        z_copy(0, k).wait_recv()
        home_copy(k).start()

    own_rows = v_pair[0:rows, :]
    share = gl_ref.shape[1]

    def latent_term(o):
        at = chunk(level(tp, o, ntp), share)
        return lax.dot_general(
            own_rows, w_s[at, :], NT, preferred_element_type=jnp.float32
        ).astype(jnp.bfloat16)

    def side_copy(bit, o):
        return remote(
            gl_s.at[o], gl_recv.at[o], t_send.at[o], t_recv.at[o], sides[bit]
        )

    alive = list(range(ntp))
    moves = []
    for bit in bits:
        leaving = [o for o in alive if o & bit]
        if bit == 1:
            for o in leaving:
                gl_s[o] = latent_term(o)
                side_copy(bit, o).start()
            alive = [o for o in alive if not o & bit]
            for o in alive:
                gl_s[o] = latent_term(o)
        else:
            for o in leaving:
                side_copy(bit, o).start()
            alive = [o for o in alive if not o & bit]
        moves.append((bit, leaving, alive))
        if bit != bits[-1]:
            for o in leaving:
                side_copy(bit, o).wait_recv()
            for o in alive:
                gl_s[o] = (
                    gl_s[o].astype(jnp.float32) + gl_recv[o + bit].astype(jnp.float32)
                ).astype(jnp.bfloat16)
    for t in range(nz):
        lat_copy(t).wait_recv()
    for k in range(nz):
        home_copy(k).wait_recv()

    parts = line_send.shape[2]
    piece = width // parts

    def term(t, s):
        block = max(piece, DV)
        skip = s * piece % block
        at = pl.ds(pl.multiple_of((2 * t + y) * width + s * piece - skip, DV), block)
        own = lat_s[:, at][:, skip : skip + piece]
        other = latp_s[t, :, s * piece : (s + 1) * piece]
        return lax.dot_general(
            jnp.concatenate([own, other], axis=0), v_pair[...], TN,
            preferred_element_type=jnp.float32,
        )

    flip = z // (nz // 2)
    zz = z + flip * (nz - 1 - 2 * z)

    def line_copy(way, t, s):
        return remote(
            line_send.at[way, t, s], line_recv.at[way, t, s],
            u_send.at[way, t, s], u_recv.at[way, t, s],
            {"sp": 2 * (z + 1 - 2 * way) + y}
        )

    hops = []
    for i in range(nz - 1):
        hops += [(0, nz - 1 - i), (1, i)]
    hops = [(back, t) for back, t in hops if t < nz // 2 - 1 or not back]

    for back, tt in hops:
        way = flip + back * (1 - 2 * flip)
        t = tt + flip * (nz - 1 - 2 * tt)
        for s in range(parts):
            @pl.when((zz > tt) if back else (zz < tt))
            def _():
                sum_s[...] = term(t, s)

                def more():
                    line_copy(way, t, s).wait_recv()
                    sum_s[...] += line_recv[way, t, s].astype(jnp.float32)

                if back:
                    more()
                else:
                    pl.when(zz > 0)(more)
                line_send[way, t, s] = sum_s[...].astype(jnp.bfloat16)
                line_copy(way, t, s).start()

    last = bits[-1]
    side_copy(last, last).wait_recv()
    gl_ref[...] = (gl_s[0].astype(jnp.float32) + gl_recv[last].astype(jnp.float32)).astype(
        jnp.bfloat16
    )
    for s in range(parts):
        at = slice(s * piece, (s + 1) * piece)
        gw_ref[at, :] = term(z, s)
    for k in range(1, nz):
        z_copy(1, k).wait_recv()
        z_copy(2, k).wait_recv()
    for way in range(2):
        @pl.when((z < nz - 1) if way else (z > 0))
        def _():
            for s in range(parts):
                line_copy(way, z, s).wait_recv()
                gw_ref[s * piece : (s + 1) * piece, :] += line_recv[way, z, s].astype(jnp.float32)

    for back, tt in hops:
        way = flip + back * (1 - 2 * flip)
        t = tt + flip * (nz - 1 - 2 * tt)
        for s in range(parts):
            @pl.when((zz > tt) if back else (zz < tt))
            def _():
                line_copy(way, t, s).wait_send()
    for k in range(1, nz):
        for part in range(5):
            send(part, k).wait_send()
        for part in range(3):
            z_copy(part, k).wait_send()
    for k in range(nz):
        lat_copy(k).wait_send()
        home_copy(k).wait_send()
        y_copy(k).wait_send()
        for part in range(3):
            passed(part, k).wait_send()
    for bit, leaving, _ in moves:
        for o in leaving:
            side_copy(bit, o).wait_send()


def level_call(
    queries, keys, latents, value_weight, first, second, cotangent, lse, head_lambda, n, ntp
):
    rows = queries.shape[0]
    depth, wide = value_weight.shape
    nz = n // 2
    width, share = depth // n, depth // ntp
    parts = 4 if width % 256 == 0 else 2
    dense, exact = jnp.bfloat16, jnp.float32
    vmem = pl.BlockSpec(memory_space=pltpu.VMEM)
    hbm = pl.BlockSpec(memory_space=pl.ANY)
    sem = pltpu.SemaphoreType.DMA
    buffers = (
        [((rows, wide), dense)] * 3
        + [((rows, depth), dense), ((depth, wide), dense)]
        + [((rows, wide), dense), ((nz, 8, rows), exact), ((rows, wide), dense)]
        + [((n * rows, DV), dense)] * 2
        + [((nz, rows, DV), dense)] * 2
        + [((n, 8, rows), exact), ((n * rows // BLOCK, 8, BLOCK), exact)]
        + [((n * rows, DV), dense)] * 2
        + [((nz, rows, width), dense), ((2 * rows, DV), dense)]
        + [((2 * rows, BLOCK), exact)] * 2
        + [((rows, BLOCK), exact)] * 2
        + [((rows, DV), exact)] * 2
        + [((DV, n * rows), exact), ((n * rows, DV), exact)]
        + [((nz, rows, DV), dense)] * 5
        + [((2 * rows, wide), dense)]
        + [((ntp, rows, share), dense)] * 2
        + [((2, nz, parts, width // parts, wide), dense)] * 2
        + [((width // parts, wide), exact)]
    )
    sems = (
        [(5,), (4,), (5, nz), (5, nz), (3, nz), (3, nz), (nz,), (nz,)]
        + [(nz,), (nz,), (3, nz), (3, nz), (nz,), (nz,), (ntp,), (ntp,)]
        + [(2, nz, parts)] * 2
    )
    return pl.pallas_call(
        functools.partial(level_kernel, nz, ntp),
        out_shape=[
            jax.ShapeDtypeStruct((rows, wide), dense),
            jax.ShapeDtypeStruct((rows, wide), dense),
            jax.ShapeDtypeStruct((rows, share), dense),
            jax.ShapeDtypeStruct((width, wide), exact),
        ],
        in_specs=[hbm] * 7 + [vmem, pl.BlockSpec(memory_space=pltpu.SMEM)],
        out_specs=[vmem] * 4,
        scratch_shapes=[pltpu.VMEM(*b) for b in buffers] + [sem(s) for s in sems],
        compiler_params=pltpu.CompilerParams(collective_id=1, has_side_effects=True),
    )(queries, keys, latents, value_weight, first, second, cotangent, lse, head_lambda)


def finish_kernel(q_ref, k_ref, gl_ref, gw_ref, q_out, k_out, gl_out, gw_out):
    q_out[...] = q_ref[...].astype(jnp.float32)
    k_out[...] = k_ref[...].astype(jnp.float32)
    gl_out[...] = gl_ref[...]
    gw_out[...] = gw_ref[...]


def finish(q_home, k_home, gl, gw):
    vmem = pl.BlockSpec(memory_space=pltpu.VMEM)
    kinds = ((q_home, jnp.float32), (k_home, jnp.float32), (gl, gl.dtype), (gw, gw.dtype))
    return pl.pallas_call(
        finish_kernel,
        out_shape=[jax.ShapeDtypeStruct(a.shape, kind) for a, kind in kinds],
        in_specs=[vmem] * 4,
        out_specs=[vmem] * 4,
    )(q_home, k_home, gl, gw)


def by_level(
    queries, key_vectors, latents, value_weight, log_sums, out_first, out_second, cotangent,
    head_lambda
):
    n, ntp = lax.axis_size("sp"), lax.axis_size("tp")
    return tuple(
        finish(
            *level_call(
                queries, key_vectors, latents, value_weight, out_first, out_second, cotangent,
                log_sums.T, head_lambda, n, ntp
            )
        )
    )


def dispatch(queries, key_vectors, latents, value_weight, log_sums, *rest):
    n, ntp = lax.axis_size("sp"), lax.axis_size("tp")
    rows, depth = latents.shape
    heads = rest[-1].shape[0]
    fits = heads * 2 == n and heads & (heads - 1) == 0 and heads > 1
    fits = fits and ntp & (ntp - 1) == 0 and ntp > 1
    fits = fits and rows % 32 == 0 and (n * rows) % BLOCK == 0
    fits = fits and depth % (n * DV) == 0 and depth % (ntp * DV) == 0
    fits = fits and depth // ntp == value_weight.shape[1]
    run = by_level if fits else per_device
    return run(queries, key_vectors, latents, value_weight, log_sums, *rest)


def solution(mesh):
    return jax.shard_map(
        dispatch,
        mesh=mesh,
        in_specs=(
            P("sp", "tp"),
            P("sp", "tp"),
            P("sp", None),
            P(None, "tp"),
            P("sp", "tp"),
            P("sp", "tp"),
            P("sp", "tp"),
            P("sp", "tp"),
            P("tp"),
        ),
        out_specs=(P("sp", "tp"), P("sp", "tp"), P("sp", "tp"), P("sp", "tp")),
        check_vma=False,
    )
```

```python
import functools

import jax
import jax.numpy as jnp
from jax import lax
from jax.experimental import pallas as pl
from jax.experimental.pallas import tpu as pltpu
from jax.sharding import PartitionSpec as P

DH = 64
DV = 128
BLOCK = 256


def row_terms(out_first, out_second, cotangent, head_lambda):
    count = out_first.shape[0]
    head_count = head_lambda.shape[0]
    first = out_first.astype(jnp.float32).reshape(count, head_count, DV)
    second = out_second.astype(jnp.float32).reshape(count, head_count, DV)
    mixed = first - head_lambda[None, :, None] * second
    inverse = lax.rsqrt(jnp.mean(mixed * mixed, axis=-1, keepdims=True) + 1e-06)
    normed = mixed * inverse
    grad_out = cotangent.astype(jnp.float32).reshape(count, head_count, DV)
    grad_mixed = inverse * (grad_out - normed * jnp.mean(grad_out * normed, axis=-1, keepdims=True))
    grad_rows = grad_mixed.astype(jnp.bfloat16)
    widened = lax.optimization_barrier(grad_rows).astype(jnp.float32)
    row_dots = jnp.stack(
        [jnp.sum(widened * first, axis=-1), jnp.sum(widened * second, axis=-1)], axis=-1
    )
    return (grad_rows.reshape(count, head_count * DV), row_dots.reshape(count, head_count * 2))


def block_grads(
    query_rows, grad_rows, lse_rows, dot_rows, query_pos, key_rows, value_rows, key_pos, head_lambda
):
    count = query_rows.shape[0]
    width = key_rows.shape[0]
    head_count = head_lambda.shape[0]
    score_scale = DH ** (-0.5)
    query_heads = query_rows.reshape(count, head_count, 2, DH)
    key_heads = key_rows.reshape(width, head_count, 2, DH)
    grad_heads = grad_rows.reshape(count, head_count, DV)
    value_heads = value_rows.reshape(width, head_count, DV)
    scores = (
        jnp.einsum("nhad,mhad->hanm", query_heads, key_heads, preferred_element_type=jnp.float32)
        * score_scale
    )
    causal = query_pos[:, None] >= key_pos[None, :]
    shifts = lse_rows.reshape(count, head_count, 2).transpose(1, 2, 0)[..., None]
    probs = jnp.exp(jnp.where(causal, scores - shifts, -1e30))
    d_attn = jnp.einsum("nhe,mhe->hnm", grad_heads, value_heads, preferred_element_type=jnp.float32)
    dots = dot_rows.reshape(count, head_count, 2).transpose(1, 2, 0)[..., None]
    map_weight = jnp.stack([jnp.ones_like(head_lambda), -head_lambda], axis=1)[:, :, None, None]
    d_scores = (map_weight * probs * (d_attn[:, None] - dots)).astype(jnp.bfloat16)
    weights = (probs[:, 0] - head_lambda[:, None, None] * probs[:, 1]).astype(jnp.bfloat16)
    grad_q = (
        jnp.einsum("hanm,mhad->nhad", d_scores, key_heads, preferred_element_type=jnp.float32)
        * score_scale
    )
    grad_k = (
        jnp.einsum("hanm,nhad->mhad", d_scores, query_heads, preferred_element_type=jnp.float32)
        * score_scale
    )
    grad_v = jnp.einsum("hnm,nhe->mhe", weights, grad_heads, preferred_element_type=jnp.float32)
    return (grad_q.reshape(count, -1), grad_k.reshape(width, -1), grad_v.reshape(width, -1))


def per_device(
    queries,
    key_vectors,
    latents,
    value_weight,
    log_sums,
    out_first,
    out_second,
    cotangent,
    head_lambda,
):
    local_rows = queries.shape[0]
    offset = lax.axis_index("sp") * local_rows
    positions = offset + jnp.arange(local_rows, dtype=jnp.int32)
    last_row = offset + local_rows - 1
    values = jnp.dot(latents, value_weight, preferred_element_type=jnp.float32).astype(jnp.bfloat16)
    grad_rows, row_dots = row_terms(out_first, out_second, cotangent, head_lambda)
    gathered_stats = (
        lax.all_gather(log_sums, "sp", axis=0, tiled=True),
        lax.all_gather(row_dots, "sp", axis=0, tiled=True),
    )
    key_rows = lax.all_gather(key_vectors, "sp", axis=0, tiled=True)
    value_rows = lax.all_gather(values, "sp", axis=0, tiled=True)
    count = key_rows.shape[0]

    def compute(current):
        key_pos = jnp.arange(count, dtype=jnp.int32)
        grad_q, unused_k, unused_v = block_grads(
            queries,
            grad_rows,
            log_sums,
            row_dots,
            positions,
            key_rows,
            value_rows,
            key_pos,
            head_lambda,
        )
        return grad_q

    grad_queries = lax.cond(
        jnp.int32(0) <= last_row,
        compute,
        lambda current: current,
        jnp.zeros((local_rows, queries.shape[1]), jnp.float32),
    )
    start_totals = (
        jnp.zeros((local_rows, key_vectors.shape[1]), jnp.float32),
        jnp.zeros((local_rows, values.shape[1]), jnp.float32),
    )
    query_rows = lax.all_gather(queries, "sp", axis=0, tiled=True)
    grad_piece = lax.all_gather(grad_rows, "sp", axis=0, tiled=True)
    add_count = query_rows.shape[0]

    def compute(current):
        query_pos = jnp.arange(add_count, dtype=jnp.int32)
        lse_rows = gathered_stats[0]
        dot_rows = gathered_stats[1]
        unused_q, grad_k, grad_v = block_grads(
            query_rows,
            grad_piece,
            lse_rows,
            dot_rows,
            query_pos,
            key_vectors,
            values,
            positions,
            head_lambda,
        )
        return (grad_k, grad_v)

    grad_keys, grad_values = lax.cond(
        jnp.int32(0) + add_count - 1 >= offset, compute, lambda current: current, start_totals
    )
    values_grad = grad_values.astype(jnp.bfloat16)
    grad_weight = lax.psum_scatter(
        lax.dot_general(
            latents, values_grad, (((0,), (0,)), ((), ())), preferred_element_type=jnp.float32
        ).astype(jnp.bfloat16),
        "sp",
        scatter_dimension=0,
        tiled=True,
    ).astype(jnp.float32)
    latent_partial = lax.dot_general(
        values_grad, value_weight, (((1,), (1,)), ((), ())), preferred_element_type=jnp.float32
    )
    grad_latents = lax.psum_scatter(
        latent_partial.astype(jnp.bfloat16), "tp", scatter_dimension=1, tiled=True
    )
    return (grad_queries, grad_keys, grad_latents, grad_weight)


def level(z, k, nz):
    bit, out = 1, z
    while bit < nz:
        out = out + ((k // bit) % 2) * bit * (1 - 2 * ((z // bit) % 2))
        bit *= 2
    return out


def lanes(index, width=DV):
    return pl.ds(pl.multiple_of(index * width, width), width)


def chunk(index, rows):
    return pl.ds(pl.multiple_of(index * rows, rows), rows)


def remote(src, dst, send_sem, recv_sem, where):
    return pltpu.make_async_remote_copy(
        src_ref=src,
        dst_ref=dst,
        send_sem=send_sem,
        recv_sem=recv_sem,
        device_id=where,
        device_id_type=pl.DeviceIdType.MESH,
    )


def greet(devices):
    barrier = pltpu.get_barrier_semaphore()
    for device in devices:
        pl.semaphore_signal(
            barrier, inc=1, device_id=device, device_id_type=pl.DeviceIdType.MESH
        )
    return lambda: pl.semaphore_wait(barrier, len(devices))


NT = (((1,), (1,)), ((), ()))
TN = (((0,), (0,)), ((), ()))


def level_kernel(
    nz, ntp, q_ref, k_ref, lat_ref, w_ref, first_ref, second_ref, cot_ref, lse_ref, lambda_ref,
    q_home, k_home, gl_ref, gw_ref,
    first_s, second_s, cot_s, lat_s, w_s, grad_s, stat_s, v_s, q_all, do_all, k_all, v_all,
    stat_r, stat_t, q0_s, q1_s, latp_s, kk_s, s0_s, s1_s, a0_s, a1_s, dk_acc, dv_acc, dqt_s, dq_s,
    dqo_s, dqy_s, dqs_s, dks_s, dvs_s, v_pair, gl_s, gl_recv,
    line_send, line_recv, sum_s,
    load_sem, own_sem, send_sem, recv_sem, pass_send, pass_recv, lat_send, lat_recv,
    y_send, y_recv, z_send, z_recv, h_send, h_recv, t_send, t_recv,
    u_send, u_recv
):
    sp, tp = lax.axis_index("sp"), lax.axis_index("tp")
    z, y = sp // 2, lax.rem(sp, 2)
    rows = q_ref.shape[0]
    width = latp_s.shape[2]
    partner = {"sp": 2 * z + 1 - y}
    peers = [{"sp": 2 * level(z, k, nz) + y} for k in range(1, nz)]
    bits = [1 << b for b in range(ntp.bit_length() - 1)]
    sides = {bit: {"tp": level(tp, bit, ntp)} for bit in bits}
    loads = [
        pltpu.make_async_copy(src, dst, load_sem.at[i])
        for i, (src, dst) in enumerate(
            [(first_ref, first_s), (second_ref, second_s), (cot_ref, cot_s), (lat_ref, lat_s),
             (w_ref, w_s)]
        )
    ]
    for load in loads:
        load.start()
    arrived = greet(peers + [partner] + list(sides.values()))
    own_q = pltpu.make_async_copy(
        q_ref.at[:, lanes(z)], q_all.at[chunk(sp, rows)], own_sem.at[0]
    )
    own_k = pltpu.make_async_copy(k_ref.at[:, lanes(z)], k_all.at[z], own_sem.at[1])
    own_q.start()
    own_k.start()
    dqt_s[...] = jnp.zeros_like(dqt_s)
    arrived()

    def send(part, k):
        to = level(z, k, nz)
        src, dst = {
            0: (q_ref.at[:, lanes(to)], q_all.at[chunk(sp, rows)]),
            1: (grad_s.at[:, lanes(to)], do_all.at[chunk(sp, rows)]),
            2: (stat_s.at[to], stat_r.at[sp]),
            3: (k_ref.at[:, lanes(to)], k_all.at[z]),
            4: (v_s.at[:, lanes(to)], v_all.at[z]),
        }[part]
        return remote(src, dst, send_sem.at[part, k], recv_sem.at[part, k], peers[k - 1])

    def passed(part, k, own=None):
        at = 2 * level(z, k, nz) + y
        kept = (q_all, do_all, stat_r)[part].at[at if part == 2 else chunk(at, rows)]
        src = kept if own is None else own
        return remote(src, kept, pass_send.at[part, k], pass_recv.at[part, k], partner)

    def lat_copy(t):
        return remote(
            lat_ref.at[:, lanes(2 * t + 1 - y, width)], latp_s.at[t],
            lat_send.at[t], lat_recv.at[t], partner
        )

    for k in range(1, nz):
        send(0, k).start()
    passed(0, 0, q_ref.at[:, lanes(z)]).start()
    for load in loads[:3]:
        load.wait()
    columns = []
    for head in range(nz):
        at = slice(head * DV, (head + 1) * DV)
        first = first_s[:, at].astype(jnp.float32)
        second = second_s[:, at].astype(jnp.float32)
        mixed = first - lambda_ref[head] * second
        inverse = lax.rsqrt(jnp.mean(mixed * mixed, axis=-1, keepdims=True) + 1e-06)
        normed = mixed * inverse
        grad_out = cot_s[:, at].astype(jnp.float32)
        mean_dot = jnp.mean(grad_out * normed, axis=-1, keepdims=True)
        grad_rows = (inverse * (grad_out - normed * mean_dot)).astype(jnp.bfloat16)
        grad_s[:, at] = grad_rows
        widened = grad_rows.astype(jnp.float32)
        columns.append(jnp.sum(widened * first, axis=-1, keepdims=True))
        columns.append(jnp.sum(widened * second, axis=-1, keepdims=True))
    dots = jnp.concatenate(columns, axis=1).T
    for head in range(nz):
        pair = slice(2 * head, 2 * head + 2)
        stat_s[head] = jnp.concatenate(
            [lse_ref[pair, :], dots[pair, :], jnp.zeros((4, rows), jnp.float32)], axis=0
        )
    for k in range(1, nz):
        for part in (2, 1):
            send(part, k).start()
    passed(2, 0, stat_s.at[z]).start()
    passed(1, 0, grad_s.at[:, lanes(z)]).start()
    own_do = pltpu.make_async_copy(
        grad_s.at[:, lanes(z)], do_all.at[chunk(sp, rows)], own_sem.at[2]
    )
    own_do.start()
    stat_r[sp] = stat_s[z]
    for load in loads[3:]:
        load.wait()
    v_s[...] = jnp.dot(lat_s[...], w_s[...], preferred_element_type=jnp.float32).astype(
        jnp.bfloat16
    )
    for k in range(1, nz):
        for part in (3, 4):
            send(part, k).start()
    own_v = pltpu.make_async_copy(v_s.at[:, lanes(z)], v_all.at[z], own_sem.at[3])
    own_v.start()
    for part in (0, 2, 1):
        for k in range(1, nz):
            send(part, k).wait_recv()
            passed(part, k).start()
    for t in range(nz):
        lat_copy(t).start()
    own_q.wait()
    own_do.wait()
    for part in range(3):
        for k in range(nz):
            passed(part, k).wait_recv()
    scale = jnp.bfloat16(DH**-0.5)
    queries = q_all[...] * scale
    half = lax.broadcasted_iota(jnp.int32, queries.shape, 1) < DH
    q0_s[...] = jnp.where(half, queries, jnp.zeros_like(queries))
    q1_s[...] = jnp.where(half, jnp.zeros_like(queries), queries)
    tiles = stat_t.shape[0]
    stats = jnp.concatenate([stat_r[c] for c in range(2 * nz)], axis=1)
    for t in range(tiles):
        stat_t[t] = stats[:, t * BLOCK : (t + 1) * BLOCK]
    weight = lambda_ref[z]

    def z_copy(part, k):
        src = (dvs_s, dks_s, dqs_s)[part].at[k]
        dst = (
            v_pair.at[0:rows, lanes(z)], k_home.at[:, lanes(z)], q_home.at[:, lanes(z)]
        )[part]
        return remote(src, dst, z_send.at[part, k], z_recv.at[part, k], peers[k - 1])

    def home_copy(k):
        head = level(z, k, nz)
        return remote(
            v_pair.at[0:rows, lanes(head)], v_pair.at[rows : 2 * rows, lanes(head)],
            h_send.at[k], h_recv.at[k], partner
        )

    for k in range(nz):
        at = level(z, k, nz)
        if k == 0:
            own_k.wait()
            own_v.wait()
        else:
            for part in (3, 4):
                send(part, k).wait_recv()
        keys = k_all[at]
        keys_t = keys.T
        keys = keys * scale
        left = lax.broadcasted_iota(jnp.int32, keys.shape, 1) < DH
        kk_s[0:rows, :] = jnp.where(left, keys, jnp.zeros_like(keys))
        kk_s[rows:, :] = jnp.where(left, jnp.zeros_like(keys), keys)
        dk_acc[...] = jnp.zeros_like(dk_acc)
        dv_acc[...] = jnp.zeros_like(dv_acc)
        place = 2 * at + y
        begin = (place * rows) // BLOCK

        def scores(t, held):
            query_rows = chunk(t, BLOCK)
            held[0][...] = lax.dot_general(
                kk_s[...], q_all[query_rows, :], NT, preferred_element_type=jnp.float32
            )
            held[1][...] = lax.dot_general(
                v_all[at], do_all[query_rows, :], NT, preferred_element_type=jnp.float32
            )

        def tile(t, held):
            query_rows = chunk(t, BLOCK)
            stat = stat_t[t]
            d_attn = held[1][...]
            key_at = lax.broadcasted_iota(jnp.int32, (rows, BLOCK), 0)
            query_at = lax.broadcasted_iota(jnp.int32, (rows, BLOCK), 1)
            seen = key_at - query_at <= t * BLOCK - place * rows
            p0 = jnp.exp(jnp.where(seen, held[0][:rows, :] - stat[0:1, :], -1e30))
            p1 = weight * jnp.exp(jnp.where(seen, held[0][rows:, :] - stat[1:2, :], -1e30))
            ds0 = (p0 * (d_attn - stat[2:3, :])).astype(jnp.bfloat16)
            ds1 = (p1 * (stat[3:4, :] - d_attn)).astype(jnp.bfloat16)
            w = (p0 - p1).astype(jnp.bfloat16)
            dk_acc[...] += jnp.dot(
                ds0, q0_s[query_rows, :], preferred_element_type=jnp.float32
            ) + jnp.dot(ds1, q1_s[query_rows, :], preferred_element_type=jnp.float32)
            dv_acc[...] += jnp.dot(w, do_all[query_rows, :], preferred_element_type=jnp.float32)
            columns = lanes(t, BLOCK)
            dqt_s[:DH, columns] += jnp.dot(keys_t[:DH], ds0, preferred_element_type=jnp.float32)
            dqt_s[DH:, columns] += jnp.dot(keys_t[DH:], ds1, preferred_element_type=jnp.float32)

        even, odd = (s0_s, a0_s), (s1_s, a1_s)
        scores(begin, even)

        def pair(i, carry):
            t = begin + 2 * i
            scores(t + 1, odd)
            tile(t, even)
            scores(jnp.minimum(t + 2, tiles - 1), even)
            tile(t + 1, odd)
            return carry

        lax.fori_loop(0, (tiles - begin) // 2, pair, 0)

        @pl.when((tiles - begin) % 2 == 1)
        def _():
            tile(tiles - 1, even)

        grad_v, grad_k = dv_acc[...].astype(jnp.bfloat16), dk_acc[...].astype(jnp.bfloat16)
        if k == 0:
            v_pair[0:rows, lanes(z)] = grad_v
            k_home[:, lanes(z)] = grad_k
            home_copy(0).start()
        else:
            dvs_s[k] = grad_v
            z_copy(0, k).start()
            dks_s[k] = grad_k
            z_copy(1, k).start()

    def y_copy(k):
        at = level(z, k, nz)
        return remote(dqo_s.at[at], dqy_s.at[at], y_send.at[k], y_recv.at[k], partner)

    order = list(range(1, nz)) + [0]
    for t in range(tiles):
        at = slice(t * BLOCK, (t + 1) * BLOCK)
        dq_s[at, :] = (dqt_s[:, at] * DH ** (-0.5)).T
    for k in order:
        at = level(z, k, nz)
        dqo_s[at] = dq_s[chunk(2 * at + 1 - y, rows), :].astype(jnp.bfloat16)
        y_copy(k).start()
    for k in range(1, nz - 1):
        z_copy(0, k).wait_recv()
        home_copy(k).start()
    for k in order:
        at = level(z, k, nz)
        y_copy(k).wait_recv()
        added = dq_s[chunk(2 * at + y, rows), :] + dqy_s[at].astype(jnp.float32)
        if k == 0:
            q_home[:, lanes(z)] = added.astype(jnp.bfloat16)
        else:
            dqs_s[k] = added.astype(jnp.bfloat16)
            z_copy(2, k).start()
    for k in range(nz - 1, nz):
        z_copy(0, k).wait_recv()
        home_copy(k).start()

    own_rows = v_pair[0:rows, :]
    share = gl_ref.shape[1]

    def latent_term(o):
        at = chunk(level(tp, o, ntp), share)
        return lax.dot_general(
            own_rows, w_s[at, :], NT, preferred_element_type=jnp.float32
        ).astype(jnp.bfloat16)

    def side_copy(bit, o):
        return remote(
            gl_s.at[o], gl_recv.at[o], t_send.at[o], t_recv.at[o], sides[bit]
        )

    moves, alive = [], list(range(ntp))
    for bit in bits:
        moves.append((bit, [o for o in alive if o & bit]))
        alive = [o for o in alive if not o & bit]
    for o in moves[0][1]:
        gl_s[o] = latent_term(o)
        side_copy(1, o).start()
    for o in range(0, ntp, 2):
        gl_s[o] = latent_term(o)

    def later_sides():
        for (before, came), (bit, leaving) in zip(moves, moves[1:]):
            for o in came:
                side_copy(before, o).wait_recv()
                gl_s[o - before] = (
                    gl_s[o - before].astype(jnp.float32) + gl_recv[o].astype(jnp.float32)
                ).astype(jnp.bfloat16)
            for o in leaving:
                side_copy(bit, o).start()

    for t in range(nz):
        lat_copy(t).wait_recv()
    for k in range(nz):
        home_copy(k).wait_recv()

    parts = line_send.shape[2]
    piece = width // parts

    def term(t, s):
        block = max(piece, DV)
        skip = s * piece % block
        at = pl.ds(pl.multiple_of((2 * t + y) * width + s * piece - skip, DV), block)
        own = lat_s[:, at][:, skip : skip + piece]
        other = latp_s[t, :, s * piece : (s + 1) * piece]
        return lax.dot_general(
            jnp.concatenate([own, other], axis=0), v_pair[...], TN,
            preferred_element_type=jnp.float32,
        )

    flip = z // (nz // 2)
    zz = z + flip * (nz - 1 - 2 * z)

    def line_copy(way, t, s):
        return remote(
            line_send.at[way, t, s], line_recv.at[way, t, s],
            u_send.at[way, t, s], u_recv.at[way, t, s],
            {"sp": 2 * (z + 1 - 2 * way) + y}
        )

    hops = []
    for i in range(nz - 1):
        hops += [(0, nz - 1 - i), (1, i)]
    hops = [(back, t) for back, t in hops if t < nz // 2 - 1 or not back]

    for back, tt in hops:
        way = flip + back * (1 - 2 * flip)
        t = tt + flip * (nz - 1 - 2 * tt)
        for s in range(parts):
            @pl.when((zz > tt) if back else (zz < tt))
            def _():
                sum_s[...] = term(t, s)

                def more():
                    line_copy(way, t, s).wait_recv()
                    sum_s[...] += line_recv[way, t, s].astype(jnp.float32)

                if back:
                    more()
                else:
                    pl.when(zz > 0)(more)
                line_send[way, t, s] = sum_s[...].astype(jnp.bfloat16)
                line_copy(way, t, s).start()

        if (back, tt) == hops[0]:
            later_sides()

    last = bits[-1]
    side_copy(last, last).wait_recv()
    gl_ref[...] = (gl_s[0].astype(jnp.float32) + gl_recv[last].astype(jnp.float32)).astype(
        jnp.bfloat16
    )
    for s in range(parts):
        at = slice(s * piece, (s + 1) * piece)
        gw_ref[at, :] = term(z, s)
    for k in range(1, nz):
        z_copy(1, k).wait_recv()
        z_copy(2, k).wait_recv()
    for way in range(2):
        @pl.when((z < nz - 1) if way else (z > 0))
        def _():
            for s in range(parts):
                line_copy(way, z, s).wait_recv()
                gw_ref[s * piece : (s + 1) * piece, :] += line_recv[way, z, s].astype(jnp.float32)

    for back, tt in hops:
        way = flip + back * (1 - 2 * flip)
        t = tt + flip * (nz - 1 - 2 * tt)
        for s in range(parts):
            @pl.when((zz > tt) if back else (zz < tt))
            def _():
                line_copy(way, t, s).wait_send()
    for k in range(1, nz):
        for part in range(5):
            send(part, k).wait_send()
        for part in range(3):
            z_copy(part, k).wait_send()
    for k in range(nz):
        lat_copy(k).wait_send()
        home_copy(k).wait_send()
        y_copy(k).wait_send()
        for part in range(3):
            passed(part, k).wait_send()
    for bit, leaving in moves:
        for o in leaving:
            side_copy(bit, o).wait_send()


def level_call(
    queries, keys, latents, value_weight, first, second, cotangent, lse, head_lambda, n, ntp
):
    rows = queries.shape[0]
    depth, wide = value_weight.shape
    nz = n // 2
    width, share = depth // n, depth // ntp
    parts = 4 if width % 256 == 0 else 2
    dense, exact = jnp.bfloat16, jnp.float32
    vmem = pl.BlockSpec(memory_space=pltpu.VMEM)
    hbm = pl.BlockSpec(memory_space=pl.ANY)
    sem = pltpu.SemaphoreType.DMA
    buffers = (
        [((rows, wide), dense)] * 3
        + [((rows, depth), dense), ((depth, wide), dense)]
        + [((rows, wide), dense), ((nz, 8, rows), exact), ((rows, wide), dense)]
        + [((n * rows, DV), dense)] * 2
        + [((nz, rows, DV), dense)] * 2
        + [((n, 8, rows), exact), ((n * rows // BLOCK, 8, BLOCK), exact)]
        + [((n * rows, DV), dense)] * 2
        + [((nz, rows, width), dense), ((2 * rows, DV), dense)]
        + [((2 * rows, BLOCK), exact)] * 2
        + [((rows, BLOCK), exact)] * 2
        + [((rows, DV), exact)] * 2
        + [((DV, n * rows), exact), ((n * rows, DV), exact)]
        + [((nz, rows, DV), dense)] * 5
        + [((2 * rows, wide), dense)]
        + [((ntp, rows, share), dense)] * 2
        + [((2, nz, parts, width // parts, wide), dense)] * 2
        + [((width // parts, wide), exact)]
    )
    sems = (
        [(5,), (4,), (5, nz), (5, nz), (3, nz), (3, nz), (nz,), (nz,)]
        + [(nz,), (nz,), (3, nz), (3, nz), (nz,), (nz,), (ntp,), (ntp,)]
        + [(2, nz, parts)] * 2
    )
    return pl.pallas_call(
        functools.partial(level_kernel, nz, ntp),
        out_shape=[
            jax.ShapeDtypeStruct((rows, wide), dense),
            jax.ShapeDtypeStruct((rows, wide), dense),
            jax.ShapeDtypeStruct((rows, share), dense),
            jax.ShapeDtypeStruct((width, wide), exact),
        ],
        in_specs=[hbm] * 7 + [vmem, pl.BlockSpec(memory_space=pltpu.SMEM)],
        out_specs=[vmem] * 4,
        scratch_shapes=[pltpu.VMEM(*b) for b in buffers] + [sem(s) for s in sems],
        compiler_params=pltpu.CompilerParams(collective_id=1, has_side_effects=True),
    )(queries, keys, latents, value_weight, first, second, cotangent, lse, head_lambda)


def finish_kernel(*refs):
    ins, outs, held, wide, (in_sem, out_sem) = (
        refs[:4], refs[4:8], refs[8:12], refs[12:14], refs[14:]
    )

    def halves(i):
        rows = ins[i].shape[0] // 2
        for h in range(2):
            at = pl.ds(h * rows, rows)
            source = wide[i] if i < 2 else held[i]
            yield (
                at,
                pltpu.make_async_copy(ins[i].at[at], held[i].at[at], in_sem.at[i, h]),
                pltpu.make_async_copy(source.at[at], outs[i].at[at], out_sem.at[i, h]),
            )

    copies = [list(halves(i)) for i in range(4)]
    for group in copies:
        for _, load, _ in group:
            load.start()
    for i, group in enumerate(copies):
        for at, load, store in group:
            load.wait()
            if i < 2:
                wide[i][at, :] = held[i][at, :].astype(jnp.float32)
            store.start()
    for group in copies:
        for _, _, store in group:
            store.wait()


def finish(q_home, k_home, gl, gw):
    hbm = pl.BlockSpec(memory_space=pl.ANY)
    arrays = (q_home, k_home, gl, gw)
    exact = [pltpu.VMEM(a.shape, jnp.float32) for a in arrays[:2]]
    return pl.pallas_call(
        finish_kernel,
        out_shape=[
            jax.ShapeDtypeStruct(a.shape, kind)
            for a, kind in zip(arrays, (jnp.float32, jnp.float32, gl.dtype, gw.dtype))
        ],
        in_specs=[hbm] * 4,
        out_specs=[hbm] * 4,
        scratch_shapes=[pltpu.VMEM(a.shape, a.dtype) for a in arrays]
        + exact
        + [pltpu.SemaphoreType.DMA((4, 2))] * 2,
    )(q_home, k_home, gl, gw)


def by_level(
    queries, key_vectors, latents, value_weight, log_sums, out_first, out_second, cotangent,
    head_lambda
):
    n, ntp = lax.axis_size("sp"), lax.axis_size("tp")
    return tuple(
        finish(
            *level_call(
                queries, key_vectors, latents, value_weight, out_first, out_second, cotangent,
                log_sums.T, head_lambda, n, ntp
            )
        )
    )


def dispatch(queries, key_vectors, latents, value_weight, log_sums, *rest):
    n, ntp = lax.axis_size("sp"), lax.axis_size("tp")
    rows, depth = latents.shape
    heads = rest[-1].shape[0]
    fits = heads * 2 == n and heads & (heads - 1) == 0 and heads > 1
    fits = fits and ntp & (ntp - 1) == 0 and ntp > 1
    fits = fits and rows % 32 == 0 and (n * rows) % BLOCK == 0
    fits = fits and depth % (n * DV) == 0 and depth % (ntp * DV) == 0
    fits = fits and depth // ntp == value_weight.shape[1]
    run = by_level if fits else per_device
    return run(queries, key_vectors, latents, value_weight, log_sums, *rest)


def solution(mesh):
    return jax.shard_map(
        dispatch,
        mesh=mesh,
        in_specs=(
            P("sp", "tp"),
            P("sp", "tp"),
            P("sp", None),
            P(None, "tp"),
            P("sp", "tp"),
            P("sp", "tp"),
            P("sp", "tp"),
            P("sp", "tp"),
            P("tp"),
        ),
        out_specs=(P("sp", "tp"), P("sp", "tp"), P("sp", "tp"), P("sp", "tp")),
        check_vma=False,
    )
```
